512 devices in a mesh: ep: 32 (over z, x), tp: 16 (over y, core).
Axes of the slice: x: 4, y: 8, z: 8, core: 2. Of those that a mesh axis runs over, the one named last changes fastest.
Arguments:
- mixer_in: bfloat16 [4096, 2048], P('ep'), may hold values from -6 to 6
- mixer_gain: float32 [2048], replicated, may hold values from 0.1 to 1.9
- w_value: bfloat16 [2048, 1536], P(None, 'tp'), may hold values from -0.125 to 0.125
- w_gate: bfloat16 [2048, 1536], P(None, 'tp'), may hold values from -0.125 to 0.125
- w_taps: float32 [31, 1536], P(None, 'tp'), may hold values from -3 to 3
- channel_gain: float32 [1536], P('tp'), may hold values from 0.1 to 1.9
- w_output: bfloat16 [1536, 2048], P('tp'), may hold values from -0.15625 to 0.15625
- expert_in: bfloat16 [4096, 2048], P('ep'), may hold values from -6 to 6
- expert_gain: float32 [2048], replicated, may hold values from 0 to 8
- route_experts: int32 [4096, 4], P('ep'), may hold values from 0 to 31, all different within a row; in each aligned block of 128 rows (0 to 127, 128 to 255, ...) at most 32 rows name the same one
- route_scores: float32 [4096, 4], P('ep'), may hold values from -6 to 6
- expert_gate: bfloat16 [32, 2048, 2048], P('ep', None, 'tp'), may hold values from -0.125 to 0.125
- expert_up: bfloat16 [32, 2048, 2048], P('ep', None, 'tp'), may hold values from -0.125 to 0.125
- expert_down: bfloat16 [32, 2048, 2048], P('ep', 'tp'), may hold values from -0.125 to 0.125
Outputs:
- mixer_out: bfloat16 [4096, 2048], P('ep')
- expert_out: bfloat16 [4096, 2048], P('ep')
The draws below stay inside these ranges and needn't reach their ends.
Inputs may be any that keep to these rules, and one draw needn't show every extreme that they name: `route_experts`: each row names 4 different experts. In each aligned block of 128 rows (the rows of one index of ep) no expert is named more than 32 times, a bound that some block reaches.
All inputs are finite; a program needn't handle non-finite values.
Results may differ from the reference program's by a relative error of at most 0.02.
Values may be sent and summed in bfloat16 or wider, within the bound.
No kernel may reach another device: no remote copies, remote signals or barrier semaphores. Data moves between devices by JAX's collectives and lax.ppermute only.
A program may use at most 64 MiB of HBM per device.

```python
import math
import jax
import jax.numpy as jnp
import numpy as np
from jax import lax

D = 2048
CONV_CH = 1536
CONV_W = 31
FF = 2048
TOP_K = 4
TOK = 128
EXPERTS = 32
SEQ = 4096
CAP = 32
CH_DEV = 96
FF_DEV = 128
N_EP = 32


def draw_w_taps(key, part):
    base_key, factor_key = jax.random.split(jax.random.fold_in(key, 17))
    base_taps = jnp.clip(jax.random.normal(base_key, (CONV_W, CONV_CH), jnp.float32), -4.0, 4.0) * CONV_W ** (-0.5)
    factors = jnp.exp(jax.random.uniform(factor_key, (CONV_CH // CH_DEV,), jnp.float32, -math.log(3.0), math.log(3.0)))
    return base_taps * jnp.repeat(factors, CH_DEV)[None, :]


def draw_expert_gain(key, part):
    noise = jnp.clip(jax.random.normal(jax.random.fold_in(key, 29), (D,), jnp.float32), -3.0, 3.0)
    gain_values = 1.0 + 0.18 * noise
    return gain_values


def steps_of(rng, dims, cuts, low, largest):
    def one(dim, parts):
        steps = jax.random.uniform(jax.random.fold_in(jax.random.fold_in(rng, 6), dim), (parts,), jnp.float32, low / len(cuts), largest / len(cuts))
        return jnp.repeat(jnp.exp(steps), dims[dim] // parts).reshape((-1,) + (1,) * (len(dims) - dim - 1))

    level = one(*cuts[0])
    for cut in cuts[1:]:
        level = level * one(*cut)
    return level


def assign_block(key, own, number, rows, count, top, reach, skew):
    sequence = jax.random.permutation(key, count)
    heavy_load, ordinary = portions_of(count, rows * top, reach, skew, True), portions_of(count, rows * top, reach, skew, False)
    places = jnp.arange(count)

    def named(sizes, rotation):
        used = int((sizes > 0).sum())
        fixed = max(1, used // 4)
        moved = fixed + (places - fixed + rotation * (used - fixed)) % max(1, count - fixed)
        return jnp.zeros((count,), jnp.int32).at[sequence[jnp.where(places < fixed, places, moved)]].set(jnp.asarray(sizes, jnp.int32))

    sizes = jnp.where(number % 4 == 0, named(heavy_load, number // 4), named(ordinary, number - number // 4 - 1))
    mixed = jax.random.permutation(jax.random.fold_in(own, 3), count)
    giver, receiver = mixed[0:count // 2 * 2:2], mixed[1:count // 2 * 2:2]
    room = jnp.minimum(sizes[giver] - 1, reach - sizes[receiver]) // 2
    room = jnp.where((giver == sequence[0]) | (receiver == sequence[0]) | (sizes[receiver] == 0), 0, jnp.maximum(room, 0))
    moved = jax.random.randint(jax.random.fold_in(own, 4), (count // 2,), 0, 1 << 20) % (room + 1)
    sizes = sizes.at[giver].add(-moved).at[receiver].add(moved)
    members = jnp.searchsorted(jnp.cumsum(sizes), jnp.arange(rows * top), side="right").astype(jnp.int32)
    grid = members.reshape(top, rows).T
    grid = grid[jax.random.permutation(jax.random.fold_in(own, 1), rows)]
    rotation = jax.random.randint(jax.random.fold_in(own, 2), (rows, 1), 0, top)
    return jnp.take_along_axis(grid, (jnp.arange(top)[None, :] + rotation) % top, axis=1)


def portions_of(count, total, most, slope, full):
    weights = [(1 << 20) // math.isqrt(rank ** slope) + 1 for rank in range(1, count + 1)]
    largest = most if full else min(most, max(-(-total // count), total * weights[0] // sum(weights)))
    least = 1 if total - largest >= count - 1 else 0
    given, spare = [largest] + [least] * (count - 1), total - largest - least * (count - 1)
    while spare > 0:
        candidates = [i for i in range(1, count) if given[i] < largest] or [i for i in range(1, count) if given[i] < most]
        pool, budget = sum([weights[i] for i in candidates]), spare
        for i in candidates:
            addition = min(most - given[i], max(1, budget * weights[i] // pool), spare)
            given[i] = given[i] + addition
            spare = spare - addition
    return np.array(given)


def centred(key, shape, scale, reach, cuts=(), kind=jnp.bfloat16):
    factor_of = steps_of(key, shape, cuts, -0.22, 0.18) if cuts else 1.0
    drawn = jax.random.normal(key, shape, jnp.float32) * scale * factor_of
    return jnp.minimum(jnp.maximum(drawn, -reach), reach).astype(kind)


def setup_inputs(seed: int = 0) -> dict:
    streams_of = jax.random.split(jax.random.key(seed), 15)
    mixer_in = centred(streams_of[0], (SEQ, D), 1.0, 6.0, ((0, 32),))
    mixer_gain = jnp.clip(1.0 + 0.18 * jax.random.normal(streams_of[1], (D,), jnp.float32), 0.1, 1.9)
    w_value = centred(streams_of[2], (D, CONV_CH), D ** -0.5, 0.125, ((1, 16),))
    w_gate = centred(streams_of[3], (D, CONV_CH), D ** -0.5, 0.125, ((1, 16),))
    w_taps = draw_w_taps(jax.random.fold_in(streams_of[14], 71), 0)
    channel_gain = jnp.clip(1.0 + 0.18 * jax.random.normal(streams_of[5], (CONV_CH,), jnp.float32), 0.1, 1.9)
    w_output = centred(streams_of[6], (CONV_CH, D), CONV_CH ** -0.5, 0.15625, ((0, 16),))
    expert_in = centred(streams_of[7], (SEQ, D), 1.0, 6.0, ((0, 32),))
    expert_gain = draw_expert_gain(jax.random.fold_in(streams_of[14], 71), 0)
    route_experts_keys = jax.random.split(jax.random.fold_in(streams_of[9], 1), SEQ // TOK)
    route_experts_turns = jax.random.permutation(jax.random.fold_in(streams_of[9], 3), SEQ // TOK)
    route_experts = jax.vmap(lambda own, number: assign_block(jax.random.fold_in(streams_of[9], 2), own, number, TOK, EXPERTS, TOP_K, CAP, 1))(route_experts_keys, route_experts_turns).reshape((SEQ, TOP_K))
    route_scores = centred(streams_of[10], (SEQ, TOP_K), 1.0, 6.0, ((0, 32),), jnp.float32)
    expert_gate = centred(streams_of[11], (EXPERTS, D, FF), D ** -0.5, 0.125, ((0, 32), (2, 16)))
    expert_up = centred(streams_of[12], (EXPERTS, D, FF), D ** -0.5, 0.125, ((0, 32), (2, 16)))
    expert_down = centred(streams_of[13], (EXPERTS, FF, D), FF ** -0.5, 0.125, ((0, 32), (1, 16)))
    return {"mixer_in": mixer_in, "mixer_gain": mixer_gain, "w_value": w_value, "w_gate": w_gate, "w_taps": w_taps, "channel_gain": channel_gain, "w_output": w_output, "expert_in": expert_in, "expert_gain": expert_gain, "route_experts": route_experts, "route_scores": route_scores, "expert_gate": expert_gate, "expert_up": expert_up, "expert_down": expert_down}


epsilon = 1e-05
clamp_limit = 7.0
swish_slope = 1.702

def row_norm(inputs, gains):
    widened = inputs.astype(jnp.float32)
    row_mean = lax.optimization_barrier(jnp.mean(widened, axis=-1, keepdims=True))
    row_var = lax.optimization_barrier(jnp.mean(jnp.square(widened - row_mean), axis=-1, keepdims=True))
    return (widened - row_mean) * lax.rsqrt(row_var + epsilon) * gains

def mixer_half(mixer_in, mixer_gain, w_value, w_gate, w_taps, channel_gain, w_output):
    normed = row_norm(mixer_in, mixer_gain).astype(jnp.bfloat16)
    values = jnp.dot(normed, w_value, preferred_element_type=jnp.float32)
    gate_pre = jnp.dot(normed, w_gate, preferred_element_type=jnp.float32)
    gated_values = (values * jax.nn.sigmoid(gate_pre)).astype(jnp.bfloat16)
    extended = jnp.concatenate([jnp.zeros((CONV_W - 1, CONV_CH), jnp.bfloat16), gated_values], axis=0)
    conv_out = jnp.zeros((SEQ, CONV_CH), jnp.float32)
    for offset in range(CONV_W):
        conv_out = conv_out + extended[offset:offset + SEQ].astype(jnp.float32) * w_taps[offset]
    row_mean = lax.optimization_barrier(jnp.sum(conv_out, axis=1, keepdims=True)) / CONV_CH
    row_var = lax.optimization_barrier(jnp.sum(conv_out * conv_out, axis=1, keepdims=True)) / CONV_CH - row_mean * row_mean
    activated = jax.nn.silu((conv_out - row_mean) * lax.rsqrt(row_var + epsilon) * channel_gain).astype(jnp.bfloat16)
    summed = jnp.zeros((SEQ, D), jnp.float32)
    for block_index in range(CONV_CH // CH_DEV):
        first_col = block_index * CH_DEV
        block_term = jnp.dot(activated[:, first_col:first_col + CH_DEV], w_output[first_col:first_col + CH_DEV], preferred_element_type=jnp.float32)
        summed = summed + lax.optimization_barrier(block_term.astype(jnp.bfloat16)).astype(jnp.float32)
    return summed.astype(jnp.bfloat16)

def expert_half(expert_in, expert_gain, route_experts, route_scores, expert_gate, expert_up, expert_down):
    normed = row_norm(expert_in, expert_gain).astype(jnp.bfloat16)
    raised = jnp.exp(route_scores)
    route_weights = raised / lax.optimization_barrier(jnp.sum(raised, axis=1, keepdims=True))
    chosen = route_experts.reshape(N_EP, TOK * TOP_K).astype(jnp.int32)
    onehot = (chosen[:, :, None] == jnp.arange(EXPERTS, dtype=jnp.int32)[None, None, :]).astype(jnp.int32)
    slot_index = lax.optimization_barrier(jnp.sum((jnp.cumsum(onehot, axis=1) - onehot) * onehot, axis=2)).astype(jnp.int32)
    source = jnp.arange(N_EP, dtype=jnp.int32)[:, None]
    owner_row = (source * TOK + jnp.arange(TOK * TOP_K, dtype=jnp.int32)[None, :] // TOP_K).astype(jnp.int32)
    placed = ((chosen * N_EP + source) * CAP + slot_index).reshape(-1).astype(jnp.int32)
    slot_table = jnp.full((EXPERTS * N_EP * CAP,), SEQ, jnp.int32).at[placed].set(owner_row.reshape(-1))
    padded = jnp.concatenate([normed, jnp.zeros((1, D), jnp.bfloat16)], axis=0)

    def one_expert(operands):
        table_rows, gate_w, up_w, down_w = operands
        gathered = padded[table_rows.astype(jnp.int32)]
        gate_pre = jnp.minimum(jnp.dot(gathered, gate_w, preferred_element_type=jnp.float32), clamp_limit)
        up_pre = jnp.clip(jnp.dot(gathered, up_w, preferred_element_type=jnp.float32), -clamp_limit, clamp_limit)
        hidden = ((up_pre + 1.0) * gate_pre * jax.nn.sigmoid(swish_slope * gate_pre)).astype(jnp.bfloat16)
        summed = jnp.zeros((N_EP * CAP, D), jnp.float32)
        for block_index in range(FF // FF_DEV):
            first_col = block_index * FF_DEV
            block_term = jnp.dot(hidden[:, first_col:first_col + FF_DEV], down_w[first_col:first_col + FF_DEV], preferred_element_type=jnp.float32)
            summed = summed + lax.optimization_barrier(block_term.astype(jnp.bfloat16)).astype(jnp.float32)
        return summed.astype(jnp.bfloat16)
    expert_rows = lax.map(one_expert, (slot_table.reshape(EXPERTS, N_EP * CAP), expert_gate, expert_up, expert_down))
    picked = expert_rows.reshape(EXPERTS * N_EP * CAP, D)[placed].astype(jnp.float32).reshape(SEQ, TOP_K, D)
    return lax.optimization_barrier(jnp.sum(picked * route_weights[:, :, None], axis=1)).astype(jnp.bfloat16)

def reference(mixer_in, mixer_gain, w_value, w_gate, w_taps, channel_gain, w_output, expert_in, expert_gain, route_experts, route_scores, expert_gate, expert_up, expert_down):
    mixer_out = mixer_half(mixer_in, mixer_gain, w_value, w_gate, w_taps, channel_gain, w_output)
    expert_out = expert_half(expert_in, expert_gain, route_experts, route_scores, expert_gate, expert_up, expert_down)
    return (mixer_out, expert_out)
```

```python
import jax
import jax.numpy as jnp
from jax import lax
from jax.sharding import Mesh
from jax.sharding import PartitionSpec as P

CONV_CH = 1536
CONV_W = 31
TOP_K = 4
TP = ("yh", "yl", "c")
GROUP = 4


epsilon = 1e-05
clamp_limit = 7.0
swish_slope = 1.702


def shifted(block, axis, distance):
    devices = range(lax.axis_size(axis))
    route = [(i - distance, i) for i in devices if i - distance in devices]
    return lax.ppermute(block, axis, route)


def swapped(x, axis):
    return lax.ppermute(x, axis, [(0, 1), (1, 0)])


def exchanged(x, axis):
    return lax.all_to_all(x, axis, split_axis=0, concat_axis=0, tiled=True)


def sent_to_all(x, axis):
    copies = jnp.broadcast_to(x, (lax.axis_size(axis), *x.shape))
    return exchanged(copies, axis)


def total_over(x, axis):
    size = lax.axis_size(axis)
    parts = exchanged(x.reshape(size, x.shape[0] // size, x.shape[1]), axis)
    share = jnp.sum(parts.astype(jnp.float32), axis=0).astype(jnp.bfloat16)
    return lax.all_gather(share, axis, axis=0, tiled=True)


def row_norm(inputs, gains):
    widened = inputs.astype(jnp.float32)
    row_mean = jnp.mean(widened, axis=-1, keepdims=True)
    row_var = jnp.mean(jnp.square(widened - row_mean), axis=-1, keepdims=True)
    return (widened - row_mean) * lax.rsqrt(row_var + epsilon) * gains


def mixer_part(mixer_in, mixer_gain, w_value, w_gate, w_taps, channel_gain, w_output):
    normed = row_norm(mixer_in, mixer_gain).astype(jnp.bfloat16)
    values = jnp.dot(normed, w_value, preferred_element_type=jnp.float32)
    gate_pre = jnp.dot(normed, w_gate, preferred_element_type=jnp.float32)
    gated_values = (values * jax.nn.sigmoid(gate_pre)).astype(jnp.bfloat16)
    mixer_rows = gated_values.shape[0]
    reach_rows = CONV_W - 1
    earlier = shifted(gated_values[mixer_rows - reach_rows :], "ep", 1)
    extended = jnp.concatenate([earlier, gated_values], axis=0)
    conv_out = jnp.zeros(gated_values.shape, jnp.float32)
    for offset in range(CONV_W):
        conv_out = (
            conv_out + extended[offset : offset + mixer_rows].astype(jnp.float32) * w_taps[offset]
        )
    sums = jnp.concatenate([jnp.sum(conv_out, axis=1), jnp.sum(conv_out * conv_out, axis=1)])
    sums = jnp.sum(sent_to_all(sums[None], TP), axis=(0, 1))
    row_mean = (sums[:mixer_rows] / CONV_CH)[:, None]
    row_var = (sums[mixer_rows:] / CONV_CH)[:, None] - row_mean * row_mean
    activated = jax.nn.silu(
        (conv_out - row_mean) * lax.rsqrt(row_var + epsilon) * channel_gain
    ).astype(jnp.bfloat16)
    return jnp.dot(activated, w_output, preferred_element_type=jnp.float32).astype(jnp.bfloat16)


def local(
    mixer_in,
    mixer_gain,
    w_value,
    w_gate,
    w_taps,
    channel_gain,
    w_output,
    expert_in,
    expert_gain,
    route_experts,
    route_scores,
    expert_gate,
    expert_up,
    expert_down,
):
    rows_b, width = expert_in.shape
    experts = lax.axis_size("ep")
    capacity = 2 * rows_b * TOP_K // experts
    slots = capacity // GROUP
    member = lax.axis_index(("yl", "c"))

    gate_up = jnp.concatenate([expert_gate[0], expert_up[0]], axis=1)
    down = expert_down[0]
    gu_y, down_y = swapped(gate_up, "yl"), swapped(down, "yl")
    gu_c, down_c = swapped(gate_up, "c"), swapped(down, "c")
    gu_d, down_d = swapped(gu_y, "c"), swapped(down_y, "c")

    normed_b = row_norm(expert_in, expert_gain).astype(jnp.bfloat16)
    ids = route_experts.T
    raised = jnp.exp(route_scores).T
    route_weights = raised / jnp.sum(raised, axis=0, keepdims=True)
    names = jnp.arange(experts, dtype=jnp.int32)[:, None]
    named = jnp.stack([ids[k][None, :] == names for k in range(TOP_K)])
    chosen = jnp.any(named, axis=0)
    weights = jnp.sum(jnp.where(named, route_weights[:, None, :], 0.0), axis=0)
    order = jnp.arange(rows_b, dtype=jnp.int32)
    before = (order[:, None] < order[None, :]).astype(jnp.bfloat16)
    rank = jnp.dot(chosen.astype(jnp.bfloat16), before, preferred_element_type=jnp.float32)
    place = jnp.where(chosen, rank.astype(jnp.int32), -1)
    own_slots = member + GROUP * jnp.arange(slots, dtype=jnp.int32)
    taken = place[:, None, :] == own_slots[None, :, None]
    select = taken.astype(jnp.bfloat16).reshape(experts * slots, rows_b)
    mixing = jnp.where(taken, weights[:, None, :], 0.0).reshape(experts * slots, rows_b)
    mixing_hi = mixing.astype(jnp.bfloat16)
    mixing_lo = (mixing - mixing_hi.astype(jnp.float32)).astype(jnp.bfloat16)

    sending = jnp.dot(select, normed_b, preferred_element_type=jnp.float32).astype(jnp.bfloat16)
    arrived = exchanged(sending.reshape(experts, slots, width), "ep").reshape(-1, width)

    mixer_partial = mixer_part(
        mixer_in, mixer_gain, w_value, w_gate, w_taps, channel_gain, w_output
    )
    mixer_out = total_over(mixer_partial, TP)

    hidden = []
    for gu in (gate_up, gu_c, gu_y, gu_d):
        both = jnp.dot(arrived, gu, preferred_element_type=jnp.float32)
        half = both.shape[1] // 2
        g = jnp.minimum(both[:, :half], clamp_limit)
        u = jnp.clip(both[:, half:], -clamp_limit, clamp_limit)
        hidden.append(((u + 1.0) * g * jax.nn.sigmoid(swish_slope * g)).astype(jnp.bfloat16))
    hidden = jnp.concatenate(hidden, axis=1)
    downs = jnp.concatenate([down, down_c, down_y, down_d], axis=0)
    partial = jnp.dot(hidden, downs, preferred_element_type=jnp.float32).astype(jnp.bfloat16)
    returned = exchanged(partial.reshape(experts, slots, width), "ep").reshape(-1, width)

    def mixed(m):
        return lax.dot_general(
            m, returned, (((0,), (0,)), ((), ())), preferred_element_type=jnp.float32
        )

    combined = (mixed(mixing_hi) + mixed(mixing_lo)).astype(jnp.bfloat16)
    expert_out = total_over(combined, TP)
    return (mixer_out, expert_out)


def solution(mesh):
    split = Mesh(mesh.devices.reshape(mesh.shape["ep"], 4, 2, 2), ("ep", *TP))
    in_specs = (
        P("ep", None),
        P(),
        P(None, TP),
        P(None, TP),
        P(None, TP),
        P(TP),
        P(TP, None),
        P("ep", None),
        P(),
        P("ep", None),
        P("ep", None),
        P("ep", None, TP),
        P("ep", None, TP),
        P("ep", TP, None),
    )
    out_specs = (P("ep", None), P("ep", None))
    return jax.shard_map(local, mesh=split, in_specs=in_specs, out_specs=out_specs, check_vma=False)
```

```python
import jax
import jax.numpy as jnp
from jax import lax
from jax.experimental import pallas as pl
from jax.experimental.pallas import tpu as pltpu
from jax.sharding import Mesh
from jax.sharding import PartitionSpec as P

CONV_CH = 1536
CONV_W = 31
TOP_K = 4
BITS = ("y2", "y1", "y0", "c")
TP = BITS
GROUP = 4
EXPERTS = 32


epsilon = 1e-05
clamp_limit = 7.0
swish_slope = 1.702


def shifted(block, axis, distance):
    devices = range(lax.axis_size(axis))
    route = [(i - distance, i) for i in devices if i - distance in devices]
    return lax.ppermute(block, axis, route)


def swapped(x, axis):
    return lax.ppermute(x, axis, [(0, 1), (1, 0)])


def exchanged(x, axis):
    return lax.all_to_all(x, axis, split_axis=0, concat_axis=0, tiled=True)


def gathered(share):
    return lax.all_gather(share, TP, axis=0, tiled=True)


def total_over(x, axis):
    size = lax.axis_size(axis)
    parts = exchanged(x.reshape(size, x.shape[0] // size, x.shape[1]), axis)
    share = jnp.sum(parts.astype(jnp.float32), axis=0).astype(jnp.bfloat16)
    return gathered(share)


def halving_total(x):
    rows, width = x.shape
    sizes = [2] * len(BITS)
    for at in reversed(range(len(BITS))):
        x = x.reshape(*sizes[: at + 1], rows // 16, width)
        own = lax.axis_index(BITS[at])
        kept = lax.dynamic_index_in_dim(x, own, at, keepdims=False)
        given = lax.dynamic_index_in_dim(x, 1 - own, at, keepdims=False)
        x = kept + swapped(given.astype(jnp.bfloat16), BITS[at]).astype(jnp.float32)
    share = x.astype(jnp.bfloat16).reshape(rows // 16, width)
    return gathered(share)


def row_norm(inputs, gains):
    widened = inputs.astype(jnp.float32)
    row_mean = jnp.mean(widened, axis=-1, keepdims=True)
    row_var = jnp.mean(jnp.square(widened - row_mean), axis=-1, keepdims=True)
    return (widened - row_mean) * lax.rsqrt(row_var + epsilon) * gains


def mixer_part(mixer_in, mixer_gain, w_value, w_gate, w_taps, channel_gain, w_output):
    normed = row_norm(mixer_in, mixer_gain).astype(jnp.bfloat16)
    values = jnp.dot(normed, w_value, preferred_element_type=jnp.float32)
    gate_pre = jnp.dot(normed, w_gate, preferred_element_type=jnp.float32)
    gated_values = (values * jax.nn.sigmoid(gate_pre)).astype(jnp.bfloat16)
    mixer_rows = gated_values.shape[0]
    reach_rows = CONV_W - 1
    earlier = shifted(gated_values[mixer_rows - reach_rows :], "ep", 1)
    extended = jnp.concatenate([earlier, gated_values], axis=0)
    conv_out = jnp.zeros(gated_values.shape, jnp.float32)
    for offset in range(CONV_W):
        conv_out = (
            conv_out + extended[offset : offset + mixer_rows].astype(jnp.float32) * w_taps[offset]
        )
    sums = jnp.stack([jnp.sum(conv_out, axis=1), jnp.sum(conv_out * conv_out, axis=1)])
    everyone = lax.all_gather(sums, TP)
    sums = jnp.sum(everyone, axis=0)
    row_mean = (sums[0] / CONV_CH)[:, None]
    row_var = (sums[1] / CONV_CH)[:, None] - row_mean * row_mean
    activated = jax.nn.silu(
        (conv_out - row_mean) * lax.rsqrt(row_var + epsilon) * channel_gain
    ).astype(jnp.bfloat16)
    return jnp.dot(activated, w_output, preferred_element_type=jnp.float32)


def front_kernel(member, x_ref, gain_ref, ids_ref, scores_ref, rows_ref, hi_ref, lo_ref):
    rows = x_ref.shape[0]
    sent = rows_ref.shape[0]
    f32, bf16 = jnp.float32, jnp.bfloat16
    normed = row_norm(x_ref[...], gain_ref[...]).astype(bf16)
    experts = EXPERTS
    slots = sent // experts
    raised = [jnp.exp(scores_ref[pl.ds(k, 1), :]) for k in range(TOP_K)]
    total = raised[0] + raised[1] + raised[2] + raised[3]
    names = lax.broadcasted_iota(jnp.int32, (experts, rows), 0)
    chosen = jnp.zeros((experts, rows), f32)
    weights = jnp.zeros((experts, rows), f32)
    for k in range(TOP_K):
        named = ids_ref[pl.ds(k, 1), :] == names
        chosen = jnp.where(named, 1.0, chosen)
        weights = jnp.where(named, raised[k] / total, weights)
    earlier = lax.broadcasted_iota(jnp.int32, (rows, rows), 0)
    later = lax.broadcasted_iota(jnp.int32, (rows, rows), 1)
    before = jnp.where(earlier < later, 1.0, 0.0).astype(bf16)
    rank = jnp.dot(chosen.astype(bf16), before, preferred_element_type=f32)
    place = jnp.where(chosen > 0.0, rank, -1.0).astype(bf16)
    of_row = lax.broadcasted_iota(jnp.int32, (sent, experts), 0) // slots
    of_col = lax.broadcasted_iota(jnp.int32, (sent, experts), 1)
    spread = jnp.where(of_row == of_col, 1.0, 0.0).astype(bf16)
    weights_hi = weights.astype(bf16)
    weights_lo = (weights - weights_hi.astype(f32)).astype(bf16)
    slot = lax.broadcasted_iota(jnp.int32, (sent, rows), 0) % slots * GROUP + member[0]
    taken = jnp.dot(spread, place, preferred_element_type=f32) == slot.astype(f32)
    select = jnp.where(taken, 1.0, 0.0).astype(bf16)
    rows_ref[...] = jnp.dot(select, normed, preferred_element_type=f32).astype(bf16)
    wide_hi = jnp.dot(spread, weights_hi, preferred_element_type=f32)
    wide_lo = jnp.dot(spread, weights_lo, preferred_element_type=f32)
    hi_ref[...] = jnp.where(taken, wide_hi, 0.0).astype(bf16)
    lo_ref[...] = jnp.where(taken, wide_lo, 0.0).astype(bf16)


def front(member, x, gain, ids, scores, sent):
    rows, width = x.shape
    whole = pl.BlockSpec(memory_space=pltpu.VMEM)
    return pl.pallas_call(
        front_kernel,
        in_specs=[pl.BlockSpec(memory_space=pltpu.SMEM)] + [whole] * 4,
        out_specs=[whole] * 3,
        out_shape=[
            jax.ShapeDtypeStruct((sent, width), jnp.bfloat16),
            jax.ShapeDtypeStruct((sent, rows), jnp.bfloat16),
            jax.ShapeDtypeStruct((sent, rows), jnp.bfloat16),
        ],
        name="front",
    )(member.reshape(1), x, gain.reshape(1, width), ids, scores)


def expert_kernel(x_ref, *refs):
    gus, downs, out_ref = refs[:GROUP], refs[GROUP : 2 * GROUP], refs[2 * GROUP]
    gu_buf, down_buf, gu_sem, down_sem = refs[2 * GROUP + 1 :]
    inner = downs[0].shape[0]
    width = out_ref.shape[1]
    gu_copies = [pltpu.make_async_copy(gus[s], gu_buf.at[s], gu_sem.at[s]) for s in range(GROUP)]
    down_copies = [
        pltpu.make_async_copy(downs[s], down_buf.at[pl.ds(s * inner, inner)], down_sem.at[s])
        for s in range(GROUP)
    ]
    for copy in gu_copies + down_copies:
        copy.start()
    hidden = []
    for s in range(GROUP):
        gu_copies[s].wait()
        both = jnp.dot(x_ref[...], gu_buf[s], preferred_element_type=jnp.float32)
        g = jnp.minimum(both[:, :inner], clamp_limit)
        u = jnp.clip(both[:, inner:], -clamp_limit, clamp_limit)
        hidden.append(((u + 1.0) * g * jax.nn.sigmoid(swish_slope * g)).astype(jnp.bfloat16))
    hidden = jnp.concatenate(hidden, axis=1)
    for copy in down_copies:
        copy.wait()
    step = 512
    for at in range(0, width, step):
        out_ref[:, at : at + step] = jnp.dot(
            hidden, down_buf[:, at : at + step], preferred_element_type=jnp.float32
        ).astype(jnp.bfloat16)


def expert(x, gus, downs):
    rows, width = x.shape
    inner = downs[0].shape[0]
    whole = pl.BlockSpec(memory_space=pltpu.VMEM)
    outside = pl.BlockSpec(memory_space=pl.ANY)
    return pl.pallas_call(
        expert_kernel,
        in_specs=[whole] + [outside] * (2 * GROUP),
        out_specs=whole,
        out_shape=jax.ShapeDtypeStruct((rows, width), jnp.bfloat16),
        scratch_shapes=[
            pltpu.VMEM((GROUP, width, 2 * inner), jnp.bfloat16),
            pltpu.VMEM((GROUP * inner, width), jnp.bfloat16),
            pltpu.SemaphoreType.DMA((GROUP,)),
            pltpu.SemaphoreType.DMA((GROUP,)),
        ],
        name="expert",
    )(x, *gus, *downs)


def program(
    mixer_in,
    mixer_gain,
    w_value,
    w_gate,
    w_taps,
    channel_gain,
    w_output,
    expert_in,
    expert_gain,
    route_experts,
    route_scores,
    expert_gate,
    expert_up,
    expert_down,
):
    rows_b, width = expert_in.shape
    experts = lax.axis_size("ep")
    capacity = 2 * rows_b * TOP_K // experts
    slots = capacity // GROUP
    member = lax.axis_index(("y0", "c")).astype(jnp.int32)

    gate_up = jnp.concatenate([expert_gate[0], expert_up[0]], axis=1)
    down = expert_down[0]
    gu_y = swapped(gate_up, "y0")
    down_y = swapped(down, "y0")
    gu_c = swapped(gate_up, "c")
    down_c = swapped(down, "c")
    gu_d = swapped(gu_y, "c")
    down_d = swapped(down_y, "c")

    sending, mixing_hi, mixing_lo = front(
        member, expert_in, expert_gain, route_experts.T, route_scores.T, experts * slots
    )
    arrived = exchanged(sending.reshape(experts, slots, width), "ep").reshape(-1, width)

    mixer_partial = mixer_part(
        mixer_in, mixer_gain, w_value, w_gate, w_taps, channel_gain, w_output
    )
    mixer_out = halving_total(mixer_partial)

    partial = expert(arrived, (gate_up, gu_c, gu_y, gu_d), (down, down_c, down_y, down_d))
    returned = exchanged(partial.reshape(experts, slots, width), "ep").reshape(-1, width)

    def mixed(m):
        return lax.dot_general(
            m, returned, (((0,), (0,)), ((), ())), preferred_element_type=jnp.float32
        )

    combined = (mixed(mixing_hi) + mixed(mixing_lo)).astype(jnp.bfloat16)
    expert_out = total_over(combined, TP)
    return (mixer_out, expert_out)


def solution(mesh):
    split = Mesh(mesh.devices.reshape(mesh.shape["ep"], 2, 2, 2, 2), ("ep", *TP))
    in_specs = (
        P("ep", None),
        P(),
        P(None, TP),
        P(None, TP),
        P(None, TP),
        P(TP),
        P(TP, None),
        P("ep", None),
        P(),
        P("ep", None),
        P("ep", None),
        P("ep", None, TP),
        P("ep", None, TP),
        P("ep", TP, None),
    )
    out_specs = (P("ep", None), P("ep", None))
    return jax.shard_map(program, mesh=split, in_specs=in_specs, out_specs=out_specs, check_vma=False)
```

```python
import jax
import jax.numpy as jnp
from jax import lax
from jax.experimental import pallas as pl
from jax.experimental.pallas import tpu as pltpu
from jax.sharding import Mesh
from jax.sharding import PartitionSpec as P

CONV_CH = 1536
CONV_W = 31
TOP_K = 4
BITS = ("y2", "y1", "y0", "c")
TP = BITS
GROUP = 4
EXPERTS = 32


epsilon = 1e-05
clamp_limit = 7.0
swish_slope = 1.702


def shifted(block, axis, distance):
    devices = range(lax.axis_size(axis))
    route = [(i - distance, i) for i in devices if i - distance in devices]
    return lax.ppermute(block, axis, route)


def swapped(x, axis):
    return lax.ppermute(x, axis, [(0, 1), (1, 0)])


def exchanged(x, axis):
    return lax.all_to_all(x, axis, split_axis=0, concat_axis=0, tiled=True)


def gathered(share):
    return lax.all_gather(share, TP, axis=0, tiled=True)


def total_over(x, axis):
    size = lax.axis_size(axis)
    parts = exchanged(x.reshape(size, x.shape[0] // size, x.shape[1]), axis)
    share = jnp.sum(parts.astype(jnp.float32), axis=0).astype(jnp.bfloat16)
    return gathered(share)


def halving_total(x):
    rows, width = x.shape
    sizes = [2] * len(BITS)
    for at in reversed(range(len(BITS))):
        x = x.reshape(*sizes[: at + 1], rows // 16, width)
        own = lax.axis_index(BITS[at])
        kept = lax.dynamic_index_in_dim(x, own, at, keepdims=False)
        given = lax.dynamic_index_in_dim(x, 1 - own, at, keepdims=False)
        x = kept + swapped(given.astype(jnp.bfloat16), BITS[at]).astype(jnp.float32)
    share = x.astype(jnp.bfloat16).reshape(rows // 16, width)
    return gathered(share)


def row_norm(inputs, gains):
    widened = inputs.astype(jnp.float32)
    row_mean = jnp.mean(widened, axis=-1, keepdims=True)
    row_var = jnp.mean(jnp.square(widened - row_mean), axis=-1, keepdims=True)
    return (widened - row_mean) * lax.rsqrt(row_var + epsilon) * gains


def mixer_part(mixer_in, mixer_gain, w_value, w_gate, w_taps, channel_gain, w_output):
    normed = row_norm(mixer_in, mixer_gain).astype(jnp.bfloat16)
    values = jnp.dot(normed, w_value, preferred_element_type=jnp.float32)
    gate_pre = jnp.dot(normed, w_gate, preferred_element_type=jnp.float32)
    gated_values = (values * jax.nn.sigmoid(gate_pre)).astype(jnp.bfloat16)
    mixer_rows = gated_values.shape[0]
    reach_rows = CONV_W - 1
    earlier = shifted(gated_values[mixer_rows - reach_rows :], "ep", 1)
    extended = jnp.concatenate([earlier, gated_values], axis=0)
    conv_out = jnp.zeros(gated_values.shape, jnp.float32)
    for offset in range(CONV_W):
        conv_out = (
            conv_out + extended[offset : offset + mixer_rows].astype(jnp.float32) * w_taps[offset]
        )
    sums = jnp.stack([jnp.sum(conv_out, axis=1), jnp.sum(conv_out * conv_out, axis=1)])
    copies = jnp.broadcast_to(sums, (lax.axis_size(TP), *sums.shape))
    everyone = exchanged(copies, TP)
    sums = jnp.sum(everyone, axis=0)
    row_mean = (sums[0] / CONV_CH)[:, None]
    row_var = (sums[1] / CONV_CH)[:, None] - row_mean * row_mean
    activated = jax.nn.silu(
        (conv_out - row_mean) * lax.rsqrt(row_var + epsilon) * channel_gain
    ).astype(jnp.bfloat16)
    return jnp.dot(activated, w_output, preferred_element_type=jnp.float32)


def front_kernel(member, x_ref, gain_ref, ids_ref, scores_ref, rows_ref, hi_ref, lo_ref):
    rows = x_ref.shape[0]
    sent = rows_ref.shape[0]
    f32, bf16 = jnp.float32, jnp.bfloat16
    normed = row_norm(x_ref[...], gain_ref[...]).astype(bf16)
    experts = EXPERTS
    slots = sent // experts
    raised = [jnp.exp(scores_ref[pl.ds(k, 1), :]) for k in range(TOP_K)]
    total = raised[0] + raised[1] + raised[2] + raised[3]
    names = lax.broadcasted_iota(jnp.int32, (experts, rows), 0)
    chosen = jnp.zeros((experts, rows), f32)
    weights = jnp.zeros((experts, rows), f32)
    for k in range(TOP_K):
        named = ids_ref[pl.ds(k, 1), :] == names
        chosen = jnp.where(named, 1.0, chosen)
        weights = jnp.where(named, raised[k] / total, weights)
    earlier = lax.broadcasted_iota(jnp.int32, (rows, rows), 0)
    later = lax.broadcasted_iota(jnp.int32, (rows, rows), 1)
    before = jnp.where(earlier < later, 1.0, 0.0).astype(bf16)
    rank = jnp.dot(chosen.astype(bf16), before, preferred_element_type=f32)
    place = jnp.where(chosen > 0.0, rank, -1.0).astype(bf16)
    of_row = lax.broadcasted_iota(jnp.int32, (sent, experts), 0) // slots
    of_col = lax.broadcasted_iota(jnp.int32, (sent, experts), 1)
    spread = jnp.where(of_row == of_col, 1.0, 0.0).astype(bf16)
    weights_hi = weights.astype(bf16)
    weights_lo = (weights - weights_hi.astype(f32)).astype(bf16)
    slot = lax.broadcasted_iota(jnp.int32, (sent, rows), 0) % slots * GROUP + member[0]
    taken = jnp.dot(spread, place, preferred_element_type=f32) == slot.astype(f32)
    select = jnp.where(taken, 1.0, 0.0).astype(bf16)
    rows_ref[...] = jnp.dot(select, normed, preferred_element_type=f32).astype(bf16)
    wide_hi = jnp.dot(spread, weights_hi, preferred_element_type=f32)
    wide_lo = jnp.dot(spread, weights_lo, preferred_element_type=f32)
    hi_ref[...] = jnp.where(taken, wide_hi, 0.0).astype(bf16)
    lo_ref[...] = jnp.where(taken, wide_lo, 0.0).astype(bf16)


def front(member, x, gain, ids, scores, sent):
    rows, width = x.shape
    whole = pl.BlockSpec(memory_space=pltpu.VMEM)
    return pl.pallas_call(
        front_kernel,
        in_specs=[pl.BlockSpec(memory_space=pltpu.SMEM)] + [whole] * 4,
        out_specs=[whole] * 3,
        out_shape=[
            jax.ShapeDtypeStruct((sent, width), jnp.bfloat16),
            jax.ShapeDtypeStruct((sent, rows), jnp.bfloat16),
            jax.ShapeDtypeStruct((sent, rows), jnp.bfloat16),
        ],
        name="front",
    )(member.reshape(1), x, gain.reshape(1, width), ids, scores)


def expert_kernel(x_hbm, *refs):
    gus, downs, out_hbm = refs[:GROUP], refs[GROUP : 2 * GROUP], refs[2 * GROUP]
    x_buf, gu_buf, down_buf, out_buf, x_sem, gu_sem, down_sem, out_sem = refs[2 * GROUP + 1 :]
    inner = downs[0].shape[0]
    width = out_hbm.shape[1]
    x_copy = pltpu.make_async_copy(x_hbm, x_buf, x_sem)
    gu_copies = [pltpu.make_async_copy(gus[s], gu_buf.at[s], gu_sem.at[s]) for s in range(GROUP)]
    down_copies = [
        pltpu.make_async_copy(downs[s], down_buf.at[pl.ds(s * inner, inner)], down_sem.at[s])
        for s in range(GROUP)
    ]
    x_copy.start()
    gu_copies[0].start()
    gu_copies[1].start()
    x_copy.wait()
    hidden = []
    for s in range(GROUP):
        gu_copies[s].wait()
        if s + 2 < GROUP:
            gu_copies[s + 2].start()
        down_copies[s].start()
        both = jnp.dot(x_buf[...], gu_buf[s], preferred_element_type=jnp.float32)
        g = jnp.minimum(both[:, :inner], clamp_limit)
        u = jnp.clip(both[:, inner:], -clamp_limit, clamp_limit)
        hidden.append(((u + 1.0) * g * jax.nn.sigmoid(swish_slope * g)).astype(jnp.bfloat16))
    hidden = jnp.concatenate(hidden, axis=1)
    for copy in down_copies:
        copy.wait()
    parts = out_sem.shape[0]
    step = width // parts
    out_copies = []
    for n in range(parts):
        own = pl.ds(n * step, step)
        out_buf[:, own] = jnp.dot(
            hidden, down_buf[:, own], preferred_element_type=jnp.float32
        ).astype(jnp.bfloat16)
        copy = pltpu.make_async_copy(out_buf.at[:, own], out_hbm.at[:, own], out_sem.at[n])
        copy.start()
        out_copies.append(copy)
    for copy in out_copies:
        copy.wait()


def expert(x, gus, downs):
    rows, width = x.shape
    inner = downs[0].shape[0]
    parts = 4
    outside = pl.BlockSpec(memory_space=pl.ANY)
    return pl.pallas_call(
        expert_kernel,
        in_specs=[outside] * (1 + 2 * GROUP),
        out_specs=outside,
        out_shape=jax.ShapeDtypeStruct((rows, width), jnp.bfloat16),
        scratch_shapes=[
            pltpu.VMEM((rows, width), jnp.bfloat16),
            pltpu.VMEM((GROUP, width, 2 * inner), jnp.bfloat16),
            pltpu.VMEM((GROUP * inner, width), jnp.bfloat16),
            pltpu.VMEM((rows, width), jnp.bfloat16),
            pltpu.SemaphoreType.DMA,
            pltpu.SemaphoreType.DMA((GROUP,)),
            pltpu.SemaphoreType.DMA((GROUP,)),
            pltpu.SemaphoreType.DMA((parts,)),
        ],
        name="expert",
    )(x, *gus, *downs)


def program(
    mixer_in,
    mixer_gain,
    w_value,
    w_gate,
    w_taps,
    channel_gain,
    w_output,
    expert_in,
    expert_gain,
    route_experts,
    route_scores,
    expert_gate,
    expert_up,
    expert_down,
):
    rows_b, width = expert_in.shape
    experts = lax.axis_size("ep")
    capacity = 2 * rows_b * TOP_K // experts
    slots = capacity // GROUP
    member = lax.axis_index(("y0", "c")).astype(jnp.int32)

    gate_up = jnp.concatenate([expert_gate[0], expert_up[0]], axis=1)
    down = expert_down[0]
    gu_y = swapped(gate_up, "y0")
    down_y = swapped(down, "y0")
    gu_c = swapped(gate_up, "c")
    down_c = swapped(down, "c")
    gu_d = swapped(gu_y, "c")
    down_d = swapped(down_y, "c")

    sending, mixing_hi, mixing_lo = front(
        member, expert_in, expert_gain, route_experts.T, route_scores.T, experts * slots
    )
    arrived = exchanged(sending.reshape(experts, slots, width), "ep").reshape(-1, width)

    mixer_partial = mixer_part(
        mixer_in, mixer_gain, w_value, w_gate, w_taps, channel_gain, w_output
    )
    mixer_out = halving_total(mixer_partial)

    partial = expert(arrived, (gate_up, gu_c, gu_y, gu_d), (down, down_c, down_y, down_d))
    returned = exchanged(partial.reshape(experts, slots, width), "ep").reshape(-1, width)

    def mixed(m):
        return lax.dot_general(
            m, returned, (((0,), (0,)), ((), ())), preferred_element_type=jnp.float32
        )

    combined = (mixed(mixing_hi) + mixed(mixing_lo)).astype(jnp.bfloat16)
    expert_out = total_over(combined, TP)
    return (mixer_out, expert_out)


def solution(mesh):
    split = Mesh(mesh.devices.reshape(mesh.shape["ep"], 2, 2, 2, 2), ("ep", *TP))
    in_specs = (
        P("ep", None),
        P(),
        P(None, TP),
        P(None, TP),
        P(None, TP),
        P(TP),
        P(TP, None),
        P("ep", None),
        P(),
        P("ep", None),
        P("ep", None),
        P("ep", None, TP),
        P("ep", None, TP),
        P("ep", TP, None),
    )
    out_specs = (P("ep", None), P("ep", None))
    return jax.shard_map(program, mesh=split, in_specs=in_specs, out_specs=out_specs, check_vma=False)
```

```python
import jax
import jax.numpy as jnp
from jax import lax
from jax.experimental import pallas as pl
from jax.experimental.pallas import tpu as pltpu
from jax.sharding import Mesh
from jax.sharding import PartitionSpec as P

CONV_CH = 1536
CONV_W = 31
TOP_K = 4
BITS = ("y2", "y1", "y0", "c")
TP = BITS
GROUP = 4
EXPERTS = 32


epsilon = 1e-05
clamp_limit = 7.0
swish_slope = 1.702


def shifted(block, axis, distance):
    devices = range(lax.axis_size(axis))
    route = [(i - distance, i) for i in devices if i - distance in devices]
    return lax.ppermute(block, axis, route)


def swapped(x, axis):
    return lax.ppermute(x, axis, [(0, 1), (1, 0)])


def exchanged(x, axis):
    return lax.all_to_all(x, axis, split_axis=0, concat_axis=0, tiled=True)


def halved(x, axes):
    rows, width = x.shape
    sizes = [2] * len(axes)
    share = rows >> len(axes)
    for at in reversed(range(len(axes))):
        x = x.reshape(*sizes[: at + 1], share, width)
        own = lax.axis_index(axes[at])
        kept = lax.dynamic_index_in_dim(x, own, at, keepdims=False)
        given = lax.dynamic_index_in_dim(x, 1 - own, at, keepdims=False)
        x = kept + swapped(given.astype(jnp.bfloat16), axes[at]).astype(jnp.float32)
    return x.reshape(share, width)


def three_terms(x):
    terms = []
    for _ in range(3):
        term = x.astype(jnp.bfloat16)
        x = x - term.astype(jnp.float32)
        terms.append(term)
    return terms


def row_norm(inputs, gains):
    widened = inputs.astype(jnp.float32)
    row_mean = jnp.mean(widened, axis=-1, keepdims=True)
    row_var = jnp.mean(jnp.square(widened - row_mean), axis=-1, keepdims=True)
    return (widened - row_mean) * lax.rsqrt(row_var + epsilon) * gains


def packing_kernel(w_ref, gain_ref, out_ref):
    size, padded, step = out_ref.shape
    own = w_ref.shape[0]
    terms = three_terms(gain_ref[...])
    for block in range(size):
        out_ref[block, :own, :] = w_ref[:, block * step : (block + 1) * step]
        out_ref[block, own:, :] = jnp.zeros((padded - own, step), jnp.bfloat16)
        for at, term in enumerate(terms):
            out_ref[block, own + at : own + at + 1, :own] = term


def resharded(w_output, channel_gain):
    size = lax.axis_size(TP)
    own, width = w_output.shape
    step = width // size
    whole = pl.BlockSpec(memory_space=pltpu.VMEM)
    payload = pl.pallas_call(
        packing_kernel,
        in_specs=[whole] * 2,
        out_specs=whole,
        out_shape=jax.ShapeDtypeStruct((size, own + 8, step), jnp.bfloat16),
        name="packing",
    )(w_output, channel_gain.reshape(1, own))
    arrived = exchanged(payload, TP)
    columns = arrived[:, :own].reshape(size * own, step)
    terms = arrived[:, own : own + 3, :own].astype(jnp.float32)
    return columns, (terms[:, 0] + terms[:, 1] + terms[:, 2]).reshape(size * own, 1)


def convolved(mixer_in, mixer_gain, w_value, w_gate, w_taps):
    normed = row_norm(mixer_in, mixer_gain).astype(jnp.bfloat16)
    values = jnp.dot(normed, w_value, preferred_element_type=jnp.float32)
    gate_pre = jnp.dot(normed, w_gate, preferred_element_type=jnp.float32)
    gated_values = (values * jax.nn.sigmoid(gate_pre)).astype(jnp.bfloat16)
    mixer_rows = gated_values.shape[0]
    reach_rows = CONV_W - 1
    earlier = shifted(gated_values[mixer_rows - reach_rows :], "ep", 1)
    extended = jnp.concatenate([earlier, gated_values], axis=0)
    conv_out = jnp.zeros(gated_values.shape, jnp.float32)
    for offset in range(CONV_W):
        conv_out = (
            conv_out + extended[offset : offset + mixer_rows].astype(jnp.float32) * w_taps[offset]
        )
    return conv_out


def mixed_channels(conv_out, gains, columns):
    wide = conv_out.astype(jnp.float32)
    row_mean = jnp.sum(wide, axis=0, keepdims=True) / CONV_CH
    row_var = jnp.sum(wide * wide, axis=0, keepdims=True) / CONV_CH - row_mean * row_mean
    activated = jax.nn.silu((wide - row_mean) * lax.rsqrt(row_var + epsilon) * gains)
    return lax.dot_general(
        activated.astype(jnp.bfloat16),
        columns,
        (((0,), (0,)), ((), ())),
        preferred_element_type=jnp.float32,
    ).astype(jnp.bfloat16)


def places(ids_ref, rows):
    names = lax.broadcasted_iota(jnp.int32, (EXPERTS, rows), 0)
    named = [ids_ref[pl.ds(k, 1), :] == names for k in range(TOP_K)]
    chosen = jnp.zeros((EXPERTS, rows), jnp.float32)
    for k in range(TOP_K):
        chosen = jnp.where(named[k], 1.0, chosen)
    earlier = lax.broadcasted_iota(jnp.int32, (rows, rows), 0)
    later = lax.broadcasted_iota(jnp.int32, (rows, rows), 1)
    before = jnp.where(earlier < later, 1.0, 0.0).astype(jnp.bfloat16)
    rank = jnp.dot(chosen.astype(jnp.bfloat16), before, preferred_element_type=jnp.float32)
    return named, jnp.where(chosen > 0.0, rank, -1.0).astype(jnp.bfloat16)


def spread_over(sent, per_expert):
    of_row = lax.broadcasted_iota(jnp.int32, (sent, EXPERTS), 0) // per_expert
    of_col = lax.broadcasted_iota(jnp.int32, (sent, EXPERTS), 1)
    return jnp.where(of_row == of_col, 1.0, 0.0).astype(jnp.bfloat16)


def taken_by(place, spread, slots, member):
    sent, rows = spread.shape[0], place.shape[1]
    slot = lax.broadcasted_iota(jnp.int32, (sent, rows), 0) % slots * GROUP + member
    return jnp.dot(spread, place, preferred_element_type=jnp.float32) == slot.astype(jnp.float32)


def front_kernel(member, x_ref, gain_ref, ids_ref, rows_ref):
    rows = x_ref.shape[0]
    sent = rows_ref.shape[0]
    slots = sent // EXPERTS
    normed = row_norm(x_ref[...], gain_ref[...]).astype(jnp.bfloat16)
    _, place = places(ids_ref, rows)
    taken = taken_by(place, spread_over(sent, slots), slots, member[0])
    select = jnp.where(taken, 1.0, 0.0).astype(jnp.bfloat16)
    rows_ref[...] = jnp.dot(select, normed, preferred_element_type=jnp.float32).astype(jnp.bfloat16)


def front(member, x, gain, ids, sent):
    _, width = x.shape
    whole = pl.BlockSpec(memory_space=pltpu.VMEM)
    return pl.pallas_call(
        front_kernel,
        in_specs=[pl.BlockSpec(memory_space=pltpu.SMEM)] + [whole] * 3,
        out_specs=whole,
        out_shape=jax.ShapeDtypeStruct((sent, width), jnp.bfloat16),
        name="front",
    )(member.reshape(1), x, gain.reshape(1, width), ids)


def mixing_kernel(member, ids_ref, scores_ref, hi_ref, lo_ref):
    sent, rows = hi_ref.shape
    per_expert = sent // EXPERTS
    raised = [jnp.exp(scores_ref[pl.ds(k, 1), :]) for k in range(TOP_K)]
    total = raised[0] + raised[1] + raised[2] + raised[3]
    named, place = places(ids_ref, rows)
    weights = jnp.zeros((EXPERTS, rows), jnp.float32)
    for k in range(TOP_K):
        weights = jnp.where(named[k], raised[k] / total, weights)
    weights_hi = weights.astype(jnp.bfloat16)
    weights_lo = (weights - weights_hi.astype(jnp.float32)).astype(jnp.bfloat16)
    spread = spread_over(sent, per_expert)
    taken = taken_by(place, spread, per_expert // GROUP, member[0])
    wide_hi = jnp.dot(spread, weights_hi, preferred_element_type=jnp.float32)
    wide_lo = jnp.dot(spread, weights_lo, preferred_element_type=jnp.float32)
    hi_ref[...] = jnp.where(taken, wide_hi, 0.0).astype(jnp.bfloat16)
    lo_ref[...] = jnp.where(taken, wide_lo, 0.0).astype(jnp.bfloat16)


def mixing(member, ids, scores, sent):
    rows = ids.shape[1]
    whole = pl.BlockSpec(memory_space=pltpu.VMEM)
    return pl.pallas_call(
        mixing_kernel,
        in_specs=[pl.BlockSpec(memory_space=pltpu.SMEM)] + [whole] * 2,
        out_specs=[whole] * 2,
        out_shape=[jax.ShapeDtypeStruct((sent, rows), jnp.bfloat16)] * 2,
        name="mixing",
    )(member.reshape(1), ids, scores)


def expert_kernel(x_hbm, *refs):
    gus, downs, out_hbm = refs[:GROUP], refs[GROUP : 2 * GROUP], refs[2 * GROUP]
    x_buf, gu_buf, down_buf, out_buf, x_sem, gu_sem, down_sem, out_sem = refs[2 * GROUP + 1 :]
    inner = downs[0].shape[0]
    experts, parts, slots, step = out_hbm.shape
    x_copy = pltpu.make_async_copy(x_hbm, x_buf, x_sem)
    gu_copies = [pltpu.make_async_copy(gus[s], gu_buf.at[s], gu_sem.at[s]) for s in range(GROUP)]
    down_copies = [
        pltpu.make_async_copy(downs[s], down_buf.at[pl.ds(s * inner, inner)], down_sem.at[s])
        for s in range(GROUP)
    ]
    x_copy.start()
    gu_copies[0].start()
    gu_copies[1].start()
    x_copy.wait()
    hidden = []
    for s in range(GROUP):
        gu_copies[s].wait()
        if s + 2 < GROUP:
            gu_copies[s + 2].start()
        down_copies[s].start()
        both = jnp.dot(x_buf[...], gu_buf[s], preferred_element_type=jnp.float32)
        g = jnp.minimum(both[:, :inner], clamp_limit)
        u = jnp.clip(both[:, inner:], -clamp_limit, clamp_limit)
        hidden.append(((u + 1.0) * g * jax.nn.sigmoid(swish_slope * g)).astype(jnp.bfloat16))
    hidden = jnp.concatenate(hidden, axis=1)
    for copy in down_copies:
        copy.wait()
    out_copies = []
    for n in range(parts):
        product = jnp.dot(
            hidden, down_buf[:, n * step : (n + 1) * step], preferred_element_type=jnp.float32
        )
        out_buf[n] = product.reshape(experts, slots, step).astype(jnp.bfloat16)
        copy = pltpu.make_async_copy(out_buf.at[n], out_hbm.at[:, n], out_sem.at[n])
        copy.start()
        out_copies.append(copy)
    for copy in out_copies:
        copy.wait()


def expert(x, gus, downs):
    rows, width = x.shape
    inner = downs[0].shape[0]
    parts = GROUP
    step = width // parts
    slots = rows // EXPERTS
    outside = pl.BlockSpec(memory_space=pl.ANY)
    return pl.pallas_call(
        expert_kernel,
        in_specs=[outside] * (1 + 2 * GROUP),
        out_specs=outside,
        out_shape=jax.ShapeDtypeStruct((EXPERTS, parts, slots, step), jnp.bfloat16),
        scratch_shapes=[
            pltpu.VMEM((rows, width), jnp.bfloat16),
            pltpu.VMEM((GROUP, width, 2 * inner), jnp.bfloat16),
            pltpu.VMEM((GROUP * inner, width), jnp.bfloat16),
            pltpu.VMEM((parts, EXPERTS, slots, step), jnp.bfloat16),
            pltpu.SemaphoreType.DMA,
            pltpu.SemaphoreType.DMA((GROUP,)),
            pltpu.SemaphoreType.DMA((GROUP,)),
            pltpu.SemaphoreType.DMA((parts,)),
        ],
        name="expert",
    )(x, *gus, *downs)


def program(
    mixer_in,
    mixer_gain,
    w_value,
    w_gate,
    w_taps,
    channel_gain,
    w_output,
    expert_in,
    expert_gain,
    route_experts,
    route_scores,
    expert_gate,
    expert_up,
    expert_down,
):
    rows_b, width = expert_in.shape
    experts = lax.axis_size("ep")
    capacity = 2 * rows_b * TOP_K // experts
    slots = capacity // GROUP
    member = lax.axis_index(("y0", "c")).astype(jnp.int32)

    gate_up = jnp.concatenate([expert_gate[0], expert_up[0]], axis=1)
    down = expert_down[0]
    gu_y = swapped(gate_up, "y0")
    down_y = swapped(down, "y0")
    gu_c = swapped(gate_up, "c")
    down_c = swapped(down, "c")
    gu_d = swapped(gu_y, "c")
    down_d = swapped(down_y, "c")

    columns, gains = resharded(w_output, channel_gain)
    ids = route_experts.T
    sending = front(member, expert_in, expert_gain, ids, experts * slots)
    arrived = exchanged(sending.reshape(experts, slots, width), "ep").reshape(-1, width)

    mixing_hi, mixing_lo = mixing(member, ids, route_scores.T, experts * capacity)
    conv_out = convolved(mixer_in, mixer_gain, w_value, w_gate, w_taps)
    conv_all = lax.all_gather(conv_out.T.astype(jnp.bfloat16), TP, axis=0, tiled=True)
    mixer_share = mixed_channels(conv_all, gains, columns)
    mixer_out = lax.all_gather(mixer_share, TP)
    mixer_out = mixer_out.transpose(1, 0, 2).reshape(rows_b, width)

    partial = expert(arrived, (gate_up, gu_c, gu_y, gu_d), (down, down_c, down_y, down_d))
    wide = GROUP * experts
    returned = exchanged(partial.reshape(wide, slots, width // GROUP), ("ep", "y2", "y1"))
    returned = returned.reshape(wide * slots, width // GROUP)

    def mixed(m):
        return lax.dot_general(
            m, returned, (((0,), (0,)), ((), ())), preferred_element_type=jnp.float32
        )

    combined = mixed(mixing_hi) + mixed(mixing_lo)
    share = halved(combined, ("y0", "c")).astype(jnp.bfloat16)
    expert_out = lax.all_gather(share, TP)
    expert_out = expert_out.reshape(GROUP, rows_b, width // GROUP)
    expert_out = jnp.concatenate(list(expert_out), axis=1)
    return (mixer_out, expert_out)


def solution(mesh):
    split = Mesh(mesh.devices.reshape(mesh.shape["ep"], 2, 2, 2, 2), ("ep", *TP))
    in_specs = (
        P("ep", None),
        P(),
        P(None, TP),
        P(None, TP),
        P(None, TP),
        P(TP),
        P(TP, None),
        P("ep", None),
        P(),
        P("ep", None),
        P("ep", None),
        P("ep", None, TP),
        P("ep", None, TP),
        P("ep", TP, None),
    )
    out_specs = (P("ep", None), P("ep", None))
    return jax.shard_map(program, mesh=split, in_specs=in_specs, out_specs=out_specs, check_vma=False)
```

```python
import jax
import jax.numpy as jnp
from jax import lax
from jax.experimental import pallas as pl
from jax.experimental.pallas import tpu as pltpu
from jax.sharding import Mesh
from jax.sharding import PartitionSpec as P

CONV_CH = 1536
CONV_W = 31
TOP_K = 4
BITS = ("y2", "y1", "y0", "c")
TP = BITS
Y = BITS[:3]
GROUP = 4
EXPERTS = 32


epsilon = 1e-05
clamp_limit = 7.0
swish_slope = 1.702


def shifted(block, axis, distance):
    devices = range(lax.axis_size(axis))
    route = [(i - distance, i) for i in devices if i - distance in devices]
    return lax.ppermute(block, axis, route)


def swapped(x, axis):
    return lax.ppermute(x, axis, [(0, 1), (1, 0)])


def exchanged(x, axis):
    return lax.all_to_all(x, axis, split_axis=0, concat_axis=0, tiled=True)


def core_half(x):
    rows, width = x.shape
    x = x.reshape(2, rows // 2, width)
    own = lax.axis_index("c")
    kept = lax.dynamic_index_in_dim(x, own, 0, keepdims=False)
    given = lax.dynamic_index_in_dim(x, 1 - own, 0, keepdims=False)
    return kept + swapped(given.astype(jnp.bfloat16), "c").astype(jnp.float32)


def totals(halves):
    size = lax.axis_size(Y)
    rows, width = halves[0].shape
    share = rows // size
    parts = [half.astype(jnp.bfloat16).reshape(size, 1, share, width) for half in halves]
    arrived = exchanged(jnp.concatenate(parts, axis=1), Y)
    summed = jnp.sum(arrived.astype(jnp.float32), axis=0).astype(jnp.bfloat16)
    gathered = exchanged(jnp.broadcast_to(summed, (size, *summed.shape)), Y)
    others = swapped(gathered, "c")
    first = lax.axis_index("c") == 0
    outs = []
    for at in range(len(halves)):
        own = gathered[:, at].reshape(rows, width)
        other = others[:, at].reshape(rows, width)
        low, high = jnp.where(first, own, other), jnp.where(first, other, own)
        outs.append(jnp.concatenate([low, high], axis=0))
    return outs


def row_norm(inputs, gains):
    widened = inputs.astype(jnp.float32)
    row_mean = jnp.mean(widened, axis=-1, keepdims=True)
    row_var = jnp.mean(jnp.square(widened - row_mean), axis=-1, keepdims=True)
    return (widened - row_mean) * lax.rsqrt(row_var + epsilon) * gains


def convolved(mixer_in, mixer_gain, w_value, w_gate, w_taps):
    normed = row_norm(mixer_in, mixer_gain).astype(jnp.bfloat16)
    values = jnp.dot(normed, w_value, preferred_element_type=jnp.float32)
    gate_pre = jnp.dot(normed, w_gate, preferred_element_type=jnp.float32)
    gated_values = (values * jax.nn.sigmoid(gate_pre)).astype(jnp.bfloat16)
    mixer_rows = gated_values.shape[0]
    reach_rows = CONV_W - 1
    earlier = shifted(gated_values[mixer_rows - reach_rows :], "ep", 1)
    extended = jnp.concatenate([earlier, gated_values], axis=0)
    conv_out = jnp.zeros(gated_values.shape, jnp.float32)
    for offset in range(CONV_W):
        conv_out = (
            conv_out + extended[offset : offset + mixer_rows].astype(jnp.float32) * w_taps[offset]
        )
    return conv_out


def projected(conv_out, channel_gain, w_output):
    sums = jnp.stack([jnp.sum(conv_out, axis=1), jnp.sum(conv_out * conv_out, axis=1)])
    everyone = lax.all_gather(sums, TP)
    sums = jnp.sum(everyone, axis=0)
    row_mean = (sums[0] / CONV_CH)[:, None]
    row_var = (sums[1] / CONV_CH)[:, None] - row_mean * row_mean
    activated = jax.nn.silu(
        (conv_out - row_mean) * lax.rsqrt(row_var + epsilon) * channel_gain
    ).astype(jnp.bfloat16)
    return jnp.dot(activated, w_output, preferred_element_type=jnp.float32)


def places(ids_ref, rows):
    names = lax.broadcasted_iota(jnp.int32, (EXPERTS, rows), 0)
    named = [ids_ref[pl.ds(k, 1), :] == names for k in range(TOP_K)]
    chosen = jnp.zeros((EXPERTS, rows), jnp.float32)
    for k in range(TOP_K):
        chosen = jnp.where(named[k], 1.0, chosen)
    earlier = lax.broadcasted_iota(jnp.int32, (rows, rows), 0)
    later = lax.broadcasted_iota(jnp.int32, (rows, rows), 1)
    before = jnp.where(earlier < later, 1.0, 0.0).astype(jnp.bfloat16)
    rank = jnp.dot(chosen.astype(jnp.bfloat16), before, preferred_element_type=jnp.float32)
    return named, jnp.where(chosen > 0.0, rank, -1.0).astype(jnp.bfloat16)


def spread_over(sent, per_expert):
    of_row = lax.broadcasted_iota(jnp.int32, (sent, EXPERTS), 0) // per_expert
    of_col = lax.broadcasted_iota(jnp.int32, (sent, EXPERTS), 1)
    return jnp.where(of_row == of_col, 1.0, 0.0).astype(jnp.bfloat16)


def taken_by(place, spread, slots, member):
    sent, rows = spread.shape[0], place.shape[1]
    slot = lax.broadcasted_iota(jnp.int32, (sent, rows), 0) % slots * GROUP + member
    return jnp.dot(spread, place, preferred_element_type=jnp.float32) == slot.astype(jnp.float32)


def front_kernel(member, x_ref, gain_ref, ids_ref, rows_ref):
    rows = x_ref.shape[0]
    sent = rows_ref.shape[0]
    slots = sent // EXPERTS
    normed = row_norm(x_ref[...], gain_ref[...]).astype(jnp.bfloat16)
    _, place = places(ids_ref, rows)
    taken = taken_by(place, spread_over(sent, slots), slots, member[0])
    select = jnp.where(taken, 1.0, 0.0).astype(jnp.bfloat16)
    rows_ref[...] = jnp.dot(select, normed, preferred_element_type=jnp.float32).astype(jnp.bfloat16)


def front(member, x, gain, ids, sent):
    _, width = x.shape
    whole = pl.BlockSpec(memory_space=pltpu.VMEM)
    return pl.pallas_call(
        front_kernel,
        in_specs=[pl.BlockSpec(memory_space=pltpu.SMEM)] + [whole] * 3,
        out_specs=whole,
        out_shape=jax.ShapeDtypeStruct((sent, width), jnp.bfloat16),
        compiler_params=pltpu.CompilerParams(vmem_limit_bytes=8 << 20),
        name="front",
    )(member.reshape(1), x, gain.reshape(1, width), ids)


def mixing_kernel(member, ids_ref, scores_ref, hi_ref, lo_ref):
    sent, rows = hi_ref.shape
    slots = sent // EXPERTS
    raised = [jnp.exp(scores_ref[pl.ds(k, 1), :]) for k in range(TOP_K)]
    total = raised[0] + raised[1] + raised[2] + raised[3]
    named, place = places(ids_ref, rows)
    weights = jnp.zeros((EXPERTS, rows), jnp.float32)
    for k in range(TOP_K):
        weights = jnp.where(named[k], raised[k] / total, weights)
    weights_hi = weights.astype(jnp.bfloat16)
    weights_lo = (weights - weights_hi.astype(jnp.float32)).astype(jnp.bfloat16)
    spread = spread_over(sent, slots)
    taken = taken_by(place, spread, slots, member[0])
    wide_hi = jnp.dot(spread, weights_hi, preferred_element_type=jnp.float32)
    wide_lo = jnp.dot(spread, weights_lo, preferred_element_type=jnp.float32)
    hi_ref[...] = jnp.where(taken, wide_hi, 0.0).astype(jnp.bfloat16)
    lo_ref[...] = jnp.where(taken, wide_lo, 0.0).astype(jnp.bfloat16)


def mixing(member, ids, scores, sent):
    rows = ids.shape[1]
    whole = pl.BlockSpec(memory_space=pltpu.VMEM)
    return pl.pallas_call(
        mixing_kernel,
        in_specs=[pl.BlockSpec(memory_space=pltpu.SMEM)] + [whole] * 2,
        out_specs=[whole] * 2,
        out_shape=[jax.ShapeDtypeStruct((sent, rows), jnp.bfloat16)] * 2,
        compiler_params=pltpu.CompilerParams(vmem_limit_bytes=4 << 20),
        name="mixing",
    )(member.reshape(1), ids, scores)


def expert_kernel(x_hbm, *refs):
    gus, downs, out_hbm = refs[:GROUP], refs[GROUP : 2 * GROUP], refs[2 * GROUP]
    x_buf, gu_buf, down_buf, out_buf, x_sem, gu_sem, down_sem, out_sem = refs[2 * GROUP + 1 :]
    inner = downs[0].shape[0]
    width = out_hbm.shape[1]
    x_copy = pltpu.make_async_copy(x_hbm, x_buf, x_sem)
    gu_copies = [pltpu.make_async_copy(gus[s], gu_buf.at[s], gu_sem.at[s]) for s in range(GROUP)]
    down_copies = [
        pltpu.make_async_copy(downs[s], down_buf.at[pl.ds(s * inner, inner)], down_sem.at[s])
        for s in range(GROUP)
    ]
    x_copy.start()
    gu_copies[0].start()
    gu_copies[1].start()
    x_copy.wait()
    hidden = []
    for s in range(GROUP):
        gu_copies[s].wait()
        if s + 2 < GROUP:
            gu_copies[s + 2].start()
        down_copies[s].start()
        both = jnp.dot(x_buf[...], gu_buf[s], preferred_element_type=jnp.float32)
        g = jnp.minimum(both[:, :inner], clamp_limit)
        u = jnp.clip(both[:, inner:], -clamp_limit, clamp_limit)
        hidden.append(((u + 1.0) * g * jax.nn.sigmoid(swish_slope * g)).astype(jnp.bfloat16))
    hidden = jnp.concatenate(hidden, axis=1)
    for copy in down_copies:
        copy.wait()
    parts = out_sem.shape[0]
    step = width // parts
    out_copies = []
    for n in range(parts):
        own = pl.ds(n * step, step)
        out_buf[:, own] = jnp.dot(
            hidden, down_buf[:, own], preferred_element_type=jnp.float32
        ).astype(jnp.bfloat16)
        copy = pltpu.make_async_copy(out_buf.at[:, own], out_hbm.at[:, own], out_sem.at[n])
        copy.start()
        out_copies.append(copy)
    for copy in out_copies:
        copy.wait()


def expert(x, gus, downs):
    rows, width = x.shape
    inner = downs[0].shape[0]
    parts = 4
    outside = pl.BlockSpec(memory_space=pl.ANY)
    return pl.pallas_call(
        expert_kernel,
        in_specs=[outside] * (1 + 2 * GROUP),
        out_specs=outside,
        out_shape=jax.ShapeDtypeStruct((rows, width), jnp.bfloat16),
        scratch_shapes=[
            pltpu.VMEM((rows, width), jnp.bfloat16),
            pltpu.VMEM((GROUP, width, 2 * inner), jnp.bfloat16),
            pltpu.VMEM((GROUP * inner, width), jnp.bfloat16),
            pltpu.VMEM((rows, width), jnp.bfloat16),
            pltpu.SemaphoreType.DMA,
            pltpu.SemaphoreType.DMA((GROUP,)),
            pltpu.SemaphoreType.DMA((GROUP,)),
            pltpu.SemaphoreType.DMA((parts,)),
        ],
        compiler_params=pltpu.CompilerParams(vmem_limit_bytes=53000 << 10),
        name="expert",
    )(x, *gus, *downs)


def program(
    mixer_in,
    mixer_gain,
    w_value,
    w_gate,
    w_taps,
    channel_gain,
    w_output,
    expert_in,
    expert_gain,
    route_experts,
    route_scores,
    expert_gate,
    expert_up,
    expert_down,
):
    rows_b, width = expert_in.shape
    experts = lax.axis_size("ep")
    capacity = 2 * rows_b * TOP_K // experts
    slots = capacity // GROUP
    member = lax.axis_index(("y0", "c")).astype(jnp.int32)

    gate_up = jnp.concatenate([expert_gate[0], expert_up[0]], axis=1)
    down = expert_down[0]
    gu_y = swapped(gate_up, "y0")
    down_y = swapped(down, "y0")
    gu_c = swapped(gate_up, "c")
    down_c = swapped(down, "c")
    gu_d = swapped(gu_y, "c")
    down_d = swapped(down_y, "c")

    ids = route_experts.T
    sending = front(member, expert_in, expert_gain, ids, experts * slots)
    arrived = exchanged(sending.reshape(experts, slots, width), "ep").reshape(-1, width)

    mixing_hi, mixing_lo = mixing(member, ids, route_scores.T, experts * slots)
    conv_out = convolved(mixer_in, mixer_gain, w_value, w_gate, w_taps)
    mixer_partial = projected(conv_out, channel_gain, w_output)
    mixer_half = core_half(mixer_partial)

    partial = expert(arrived, (gate_up, gu_c, gu_y, gu_d), (down, down_c, down_y, down_d))
    returned = exchanged(partial.reshape(experts, slots, width), "ep").reshape(-1, width)

    def mixed(m):
        return lax.dot_general(
            m, returned, (((0,), (0,)), ((), ())), preferred_element_type=jnp.float32
        )

    expert_half = core_half(mixed(mixing_hi) + mixed(mixing_lo))
    mixer_out, expert_out = totals([mixer_half, expert_half])
    return (mixer_out, expert_out)


def solution(mesh):
    split = Mesh(mesh.devices.reshape(mesh.shape["ep"], 2, 2, 2, 2), ("ep", *TP))
    in_specs = (
        P("ep", None),
        P(),
        P(None, TP),
        P(None, TP),
        P(None, TP),
        P(TP),
        P(TP, None),
        P("ep", None),
        P(),
        P("ep", None),
        P("ep", None),
        P("ep", None, TP),
        P("ep", None, TP),
        P("ep", TP, None),
    )
    out_specs = (P("ep", None), P("ep", None))
    return jax.shard_map(program, mesh=split, in_specs=in_specs, out_specs=out_specs, check_vma=False)
```

```python
import jax
import jax.numpy as jnp
from jax import lax
from jax.experimental import pallas as pl
from jax.experimental.pallas import tpu as pltpu
from jax.sharding import Mesh
from jax.sharding import PartitionSpec as P

CONV_CH = 1536
CONV_W = 31
TOP_K = 4
BITS = ("y2", "y1", "y0", "c")
TP = BITS
Y = BITS[:3]
GROUP = 4
EXPERTS = 32


epsilon = 1e-05
clamp_limit = 7.0
swish_slope = 1.702


def shifted(block, axis, distance):
    devices = range(lax.axis_size(axis))
    route = [(i - distance, i) for i in devices if i - distance in devices]
    return lax.ppermute(block, axis, route)


def swapped(x, axis):
    return lax.ppermute(x, axis, [(0, 1), (1, 0)])


def exchanged(x, axis):
    return lax.all_to_all(x, axis, split_axis=0, concat_axis=0, tiled=True)


def core_half(x):
    rows, width = x.shape
    x = x.reshape(2, rows // 2, width)
    own = lax.axis_index("c")
    kept = lax.dynamic_index_in_dim(x, own, 0, keepdims=False)
    given = lax.dynamic_index_in_dim(x, 1 - own, 0, keepdims=False)
    return kept + swapped(given.astype(jnp.bfloat16), "c").astype(jnp.float32)


def totals(halves):
    size = lax.axis_size(Y)
    rows, width = halves[0].shape
    share = rows // size
    parts = [half.astype(jnp.bfloat16).reshape(size, 1, share, width) for half in halves]
    arrived = exchanged(jnp.concatenate(parts, axis=1), Y)
    summed = jnp.sum(arrived.astype(jnp.float32), axis=0).astype(jnp.bfloat16)
    gathered = exchanged(jnp.broadcast_to(summed, (size, *summed.shape)), Y)
    others = swapped(gathered, "c")
    first = lax.axis_index("c") == 0
    outs = []
    for at in range(len(halves)):
        own = gathered[:, at].reshape(rows, width)
        other = others[:, at].reshape(rows, width)
        low, high = jnp.where(first, own, other), jnp.where(first, other, own)
        outs.append(jnp.concatenate([low, high], axis=0))
    return outs


def row_norm(inputs, gains):
    widened = inputs.astype(jnp.float32)
    row_mean = jnp.mean(widened, axis=-1, keepdims=True)
    row_var = jnp.mean(jnp.square(widened - row_mean), axis=-1, keepdims=True)
    return (widened - row_mean) * lax.rsqrt(row_var + epsilon) * gains


def convolved(mixer_in, mixer_gain, w_value, w_gate, w_taps):
    normed = row_norm(mixer_in, mixer_gain).astype(jnp.bfloat16)
    values = jnp.dot(normed, w_value, preferred_element_type=jnp.float32)
    gate_pre = jnp.dot(normed, w_gate, preferred_element_type=jnp.float32)
    gated_values = (values * jax.nn.sigmoid(gate_pre)).astype(jnp.bfloat16)
    mixer_rows = gated_values.shape[0]
    reach_rows = CONV_W - 1
    earlier = shifted(gated_values[mixer_rows - reach_rows :], "ep", 1)
    extended = jnp.concatenate([earlier, gated_values], axis=0)
    conv_out = jnp.zeros(gated_values.shape, jnp.float32)
    for offset in range(CONV_W):
        conv_out = (
            conv_out + extended[offset : offset + mixer_rows].astype(jnp.float32) * w_taps[offset]
        )
    return conv_out


def projected(conv_out, channel_gain, w_output):
    sums = jnp.stack([jnp.sum(conv_out, axis=1), jnp.sum(conv_out * conv_out, axis=1)])
    everyone = lax.all_gather(sums, TP)
    sums = jnp.sum(everyone, axis=0)
    row_mean = (sums[0] / CONV_CH)[:, None]
    row_var = (sums[1] / CONV_CH)[:, None] - row_mean * row_mean
    activated = jax.nn.silu(
        (conv_out - row_mean) * lax.rsqrt(row_var + epsilon) * channel_gain
    ).astype(jnp.bfloat16)
    return jnp.dot(activated, w_output, preferred_element_type=jnp.float32)


def places(ids_ref, rows):
    names = lax.broadcasted_iota(jnp.int32, (EXPERTS, rows), 0)
    named = [ids_ref[pl.ds(k, 1), :] == names for k in range(TOP_K)]
    chosen = jnp.zeros((EXPERTS, rows), jnp.float32)
    for k in range(TOP_K):
        chosen = jnp.where(named[k], 1.0, chosen)
    earlier = lax.broadcasted_iota(jnp.int32, (rows, rows), 0)
    later = lax.broadcasted_iota(jnp.int32, (rows, rows), 1)
    before = jnp.where(earlier < later, 1.0, 0.0).astype(jnp.bfloat16)
    rank = jnp.dot(chosen.astype(jnp.bfloat16), before, preferred_element_type=jnp.float32)
    return named, jnp.where(chosen > 0.0, rank, -1.0).astype(jnp.bfloat16)


def spread_over(sent, per_expert):
    of_row = lax.broadcasted_iota(jnp.int32, (sent, EXPERTS), 0) // per_expert
    of_col = lax.broadcasted_iota(jnp.int32, (sent, EXPERTS), 1)
    return jnp.where(of_row == of_col, 1.0, 0.0).astype(jnp.bfloat16)


def taken_by(place, spread, slots, member):
    sent, rows = spread.shape[0], place.shape[1]
    slot = lax.broadcasted_iota(jnp.int32, (sent, rows), 0) % slots * GROUP + member
    return jnp.dot(spread, place, preferred_element_type=jnp.float32) == slot.astype(jnp.float32)


def front_kernel(member, x_ref, gain_ref, ids_ref, rows_ref):
    rows = x_ref.shape[0]
    sent = rows_ref.shape[0]
    slots = sent // EXPERTS
    normed = row_norm(x_ref[...], gain_ref[...]).astype(jnp.bfloat16)
    _, place = places(ids_ref, rows)
    taken = taken_by(place, spread_over(sent, slots), slots, member[0])
    select = jnp.where(taken, 1.0, 0.0).astype(jnp.bfloat16)
    rows_ref[...] = jnp.dot(select, normed, preferred_element_type=jnp.float32).astype(jnp.bfloat16)


def front(member, x, gain, ids, sent):
    _, width = x.shape
    whole = pl.BlockSpec(memory_space=pltpu.VMEM)
    return pl.pallas_call(
        front_kernel,
        in_specs=[pl.BlockSpec(memory_space=pltpu.SMEM)] + [whole] * 3,
        out_specs=whole,
        out_shape=jax.ShapeDtypeStruct((sent, width), jnp.bfloat16),
        compiler_params=pltpu.CompilerParams(vmem_limit_bytes=8 << 20),
        name="front",
    )(member.reshape(1), x, gain.reshape(1, width), ids)


def mixing_kernel(member, ids_ref, scores_ref, hi_ref, lo_ref):
    sent, rows = hi_ref.shape
    slots = sent // EXPERTS
    raised = [jnp.exp(scores_ref[pl.ds(k, 1), :]) for k in range(TOP_K)]
    total = raised[0] + raised[1] + raised[2] + raised[3]
    named, place = places(ids_ref, rows)
    weights = jnp.zeros((EXPERTS, rows), jnp.float32)
    for k in range(TOP_K):
        weights = jnp.where(named[k], raised[k] / total, weights)
    weights_hi = weights.astype(jnp.bfloat16)
    weights_lo = (weights - weights_hi.astype(jnp.float32)).astype(jnp.bfloat16)
    spread = spread_over(sent, slots)
    taken = taken_by(place, spread, slots, member[0])
    wide_hi = jnp.dot(spread, weights_hi, preferred_element_type=jnp.float32)
    wide_lo = jnp.dot(spread, weights_lo, preferred_element_type=jnp.float32)
    hi_ref[...] = jnp.where(taken, wide_hi, 0.0).astype(jnp.bfloat16)
    lo_ref[...] = jnp.where(taken, wide_lo, 0.0).astype(jnp.bfloat16)


def mixing(member, ids, scores, sent):
    rows = ids.shape[1]
    whole = pl.BlockSpec(memory_space=pltpu.VMEM)
    return pl.pallas_call(
        mixing_kernel,
        in_specs=[pl.BlockSpec(memory_space=pltpu.SMEM)] + [whole] * 2,
        out_specs=[whole] * 2,
        out_shape=[jax.ShapeDtypeStruct((sent, rows), jnp.bfloat16)] * 2,
        compiler_params=pltpu.CompilerParams(vmem_limit_bytes=4 << 20),
        name="mixing",
    )(member.reshape(1), ids, scores)


def expert_kernel(x_ref, *refs):
    gus, downs, out_ref = refs[:GROUP], refs[GROUP : 2 * GROUP], refs[2 * GROUP]
    inner = downs[0].shape[0]
    width = out_ref.shape[1]
    hidden = []
    for gu in gus:
        both = jnp.dot(x_ref[...], gu[...], preferred_element_type=jnp.float32)
        g = jnp.minimum(both[:, :inner], clamp_limit)
        u = jnp.clip(both[:, inner:], -clamp_limit, clamp_limit)
        hidden.append(((u + 1.0) * g * jax.nn.sigmoid(swish_slope * g)).astype(jnp.bfloat16))
    hidden = jnp.concatenate(hidden, axis=1)
    step = 512
    for at in range(0, width, step):
        weights = jnp.concatenate([down[:, at : at + step] for down in downs], axis=0)
        out_ref[:, at : at + step] = jnp.dot(
            hidden, weights, preferred_element_type=jnp.float32
        ).astype(jnp.bfloat16)


def expert(x, gus, downs):
    whole = pl.BlockSpec(memory_space=pltpu.VMEM)
    return pl.pallas_call(
        expert_kernel,
        in_specs=[whole] * (1 + 2 * GROUP),
        out_specs=whole,
        out_shape=jax.ShapeDtypeStruct(x.shape, jnp.bfloat16),
        compiler_params=pltpu.CompilerParams(vmem_limit_bytes=53000 << 10),
        name="expert",
    )(x, *gus, *downs)


def program(
    mixer_in,
    mixer_gain,
    w_value,
    w_gate,
    w_taps,
    channel_gain,
    w_output,
    expert_in,
    expert_gain,
    route_experts,
    route_scores,
    expert_gate,
    expert_up,
    expert_down,
):
    rows_b, width = expert_in.shape
    experts = lax.axis_size("ep")
    capacity = 2 * rows_b * TOP_K // experts
    slots = capacity // GROUP
    member = lax.axis_index(("y0", "c")).astype(jnp.int32)

    gate_up = jnp.concatenate([expert_gate[0], expert_up[0]], axis=1)
    down = expert_down[0]
    gu_y = swapped(gate_up, "y0")
    down_y = swapped(down, "y0")
    gu_c = swapped(gate_up, "c")
    down_c = swapped(down, "c")
    gu_d = swapped(gu_y, "c")
    down_d = swapped(down_y, "c")

    ids = route_experts.T
    sending = front(member, expert_in, expert_gain, ids, experts * slots)
    arrived = exchanged(sending.reshape(experts, slots, width), "ep").reshape(-1, width)

    mixing_hi, mixing_lo = mixing(member, ids, route_scores.T, experts * slots)
    conv_out = convolved(mixer_in, mixer_gain, w_value, w_gate, w_taps)
    mixer_partial = projected(conv_out, channel_gain, w_output)
    mixer_half = core_half(mixer_partial)

    partial = expert(arrived, (gate_up, gu_c, gu_y, gu_d), (down, down_c, down_y, down_d))
    returned = exchanged(partial.reshape(experts, slots, width), "ep").reshape(-1, width)

    def mixed(m):
        return lax.dot_general(
            m, returned, (((0,), (0,)), ((), ())), preferred_element_type=jnp.float32
        )

    expert_half = core_half(mixed(mixing_hi) + mixed(mixing_lo))
    mixer_out, expert_out = totals([mixer_half, expert_half])
    return (mixer_out, expert_out)


def solution(mesh):
    split = Mesh(mesh.devices.reshape(mesh.shape["ep"], 2, 2, 2, 2), ("ep", *TP))
    in_specs = (
        P("ep", None),
        P(),
        P(None, TP),
        P(None, TP),
        P(None, TP),
        P(TP),
        P(TP, None),
        P("ep", None),
        P(),
        P("ep", None),
        P("ep", None),
        P("ep", None, TP),
        P("ep", None, TP),
        P("ep", TP, None),
    )
    out_specs = (P("ep", None), P("ep", None))
    return jax.shard_map(program, mesh=split, in_specs=in_specs, out_specs=out_specs, check_vma=False)
```

```python
import jax
import jax.numpy as jnp
from jax import lax
from jax.experimental import pallas as pl
from jax.experimental.pallas import tpu as pltpu
from jax.sharding import Mesh
from jax.sharding import PartitionSpec as P

CONV_CH = 1536
CONV_W = 31
TOP_K = 4
BITS = ("y2", "y1", "y0", "c")
TP = BITS
Y = BITS[:3]
GROUP = 4
EXPERTS = 32


epsilon = 1e-05
clamp_limit = 7.0
swish_slope = 1.702


def shifted(block, axis, distance):
    devices = range(lax.axis_size(axis))
    route = [(i - distance, i) for i in devices if i - distance in devices]
    return lax.ppermute(block, axis, route)


def swapped(x, axis):
    return lax.ppermute(x, axis, [(0, 1), (1, 0)])


def exchanged(x, axis):
    return lax.all_to_all(x, axis, split_axis=0, concat_axis=0, tiled=True)


def core_half(x):
    rows, width = x.shape
    x = x.reshape(2, rows // 2, width)
    own = lax.axis_index("c")
    kept = lax.dynamic_index_in_dim(x, own, 0, keepdims=False)
    given = lax.dynamic_index_in_dim(x, 1 - own, 0, keepdims=False)
    return kept + swapped(given.astype(jnp.bfloat16), "c").astype(jnp.float32)


def totals(halves):
    size = lax.axis_size(Y)
    rows, width = halves[0].shape
    share = rows // size
    parts = [half.astype(jnp.bfloat16).reshape(size, 1, share, width) for half in halves]
    arrived = exchanged(jnp.concatenate(parts, axis=1), Y)
    summed = jnp.sum(arrived.astype(jnp.float32), axis=0).astype(jnp.bfloat16)
    gathered = exchanged(jnp.broadcast_to(summed, (size, *summed.shape)), Y)
    others = swapped(gathered, "c")
    first = lax.axis_index("c") == 0
    outs = []
    for at in range(len(halves)):
        own = gathered[:, at].reshape(rows, width)
        other = others[:, at].reshape(rows, width)
        low, high = jnp.where(first, own, other), jnp.where(first, other, own)
        outs.append(jnp.concatenate([low, high], axis=0))
    return outs


def row_norm(inputs, gains):
    widened = inputs.astype(jnp.float32)
    row_mean = jnp.mean(widened, axis=-1, keepdims=True)
    row_var = jnp.mean(jnp.square(widened - row_mean), axis=-1, keepdims=True)
    return (widened - row_mean) * lax.rsqrt(row_var + epsilon) * gains


def convolved(mixer_in, mixer_gain, w_value, w_gate, w_taps):
    normed = row_norm(mixer_in, mixer_gain).astype(jnp.bfloat16)
    values = jnp.dot(normed, w_value, preferred_element_type=jnp.float32)
    gate_pre = jnp.dot(normed, w_gate, preferred_element_type=jnp.float32)
    gated_values = (values * jax.nn.sigmoid(gate_pre)).astype(jnp.bfloat16)
    mixer_rows = gated_values.shape[0]
    reach_rows = CONV_W - 1
    earlier = shifted(gated_values[mixer_rows - reach_rows :], "ep", 1)
    extended = jnp.concatenate([earlier, gated_values], axis=0)
    conv_out = jnp.zeros(gated_values.shape, jnp.float32)
    for offset in range(CONV_W):
        conv_out = (
            conv_out + extended[offset : offset + mixer_rows].astype(jnp.float32) * w_taps[offset]
        )
    return conv_out


def projected(conv_out, channel_gain, w_output):
    sums = jnp.stack([jnp.sum(conv_out, axis=1), jnp.sum(conv_out * conv_out, axis=1)])
    everyone = lax.all_gather(sums, TP)
    sums = jnp.sum(everyone, axis=0)
    row_mean = (sums[0] / CONV_CH)[:, None]
    row_var = (sums[1] / CONV_CH)[:, None] - row_mean * row_mean
    activated = jax.nn.silu(
        (conv_out - row_mean) * lax.rsqrt(row_var + epsilon) * channel_gain
    ).astype(jnp.bfloat16)
    return jnp.dot(activated, w_output, preferred_element_type=jnp.float32)


def places(ids_ref, rows):
    names = lax.broadcasted_iota(jnp.int32, (EXPERTS, rows), 0)
    named = [ids_ref[pl.ds(k, 1), :] == names for k in range(TOP_K)]
    chosen = jnp.zeros((EXPERTS, rows), jnp.float32)
    for k in range(TOP_K):
        chosen = jnp.where(named[k], 1.0, chosen)
    earlier = lax.broadcasted_iota(jnp.int32, (rows, rows), 0)
    later = lax.broadcasted_iota(jnp.int32, (rows, rows), 1)
    before = jnp.where(earlier < later, 1.0, 0.0).astype(jnp.bfloat16)
    rank = jnp.dot(chosen.astype(jnp.bfloat16), before, preferred_element_type=jnp.float32)
    return named, jnp.where(chosen > 0.0, rank, -1.0).astype(jnp.bfloat16)


def spread_over(sent, per_expert):
    of_row = lax.broadcasted_iota(jnp.int32, (sent, EXPERTS), 0) // per_expert
    of_col = lax.broadcasted_iota(jnp.int32, (sent, EXPERTS), 1)
    return jnp.where(of_row == of_col, 1.0, 0.0).astype(jnp.bfloat16)


def taken_by(place, spread, slots, member):
    sent, rows = spread.shape[0], place.shape[1]
    slot = lax.broadcasted_iota(jnp.int32, (sent, rows), 0) % slots * GROUP + member
    return jnp.dot(spread, place, preferred_element_type=jnp.float32) == slot.astype(jnp.float32)


def front_kernel(member, x_ref, gain_ref, ids_ref, gate_ref, up_ref, rows_ref, both_ref):
    rows = x_ref.shape[0]
    inner = gate_ref.shape[1]
    both_ref[:, :inner] = gate_ref[...]
    both_ref[:, inner:] = up_ref[...]
    sent = rows_ref.shape[0]
    slots = sent // EXPERTS
    normed = row_norm(x_ref[...], gain_ref[...]).astype(jnp.bfloat16)
    _, place = places(ids_ref, rows)
    taken = taken_by(place, spread_over(sent, slots), slots, member[0])
    select = jnp.where(taken, 1.0, 0.0).astype(jnp.bfloat16)
    rows_ref[...] = jnp.dot(select, normed, preferred_element_type=jnp.float32).astype(jnp.bfloat16)


def front(member, x, gain, ids, gate, up, sent):
    _, width = x.shape
    inner = gate.shape[1]
    whole = pl.BlockSpec(memory_space=pltpu.VMEM)
    return pl.pallas_call(
        front_kernel,
        in_specs=[pl.BlockSpec(memory_space=pltpu.SMEM)] + [whole] * 5,
        out_specs=[whole] * 2,
        out_shape=[
            jax.ShapeDtypeStruct((sent, width), jnp.bfloat16),
            jax.ShapeDtypeStruct((width, 2 * inner), jnp.bfloat16),
        ],
        compiler_params=pltpu.CompilerParams(vmem_limit_bytes=57000 << 10),
        name="front",
    )(member.reshape(1), x, gain.reshape(1, width), ids, gate, up)


def mixing_kernel(member, ids_ref, scores_ref, hi_ref, lo_ref):
    sent, rows = hi_ref.shape
    slots = sent // EXPERTS
    raised = [jnp.exp(scores_ref[pl.ds(k, 1), :]) for k in range(TOP_K)]
    total = raised[0] + raised[1] + raised[2] + raised[3]
    named, place = places(ids_ref, rows)
    weights = jnp.zeros((EXPERTS, rows), jnp.float32)
    for k in range(TOP_K):
        weights = jnp.where(named[k], raised[k] / total, weights)
    weights_hi = weights.astype(jnp.bfloat16)
    weights_lo = (weights - weights_hi.astype(jnp.float32)).astype(jnp.bfloat16)
    spread = spread_over(sent, slots)
    taken = taken_by(place, spread, slots, member[0])
    wide_hi = jnp.dot(spread, weights_hi, preferred_element_type=jnp.float32)
    wide_lo = jnp.dot(spread, weights_lo, preferred_element_type=jnp.float32)
    hi_ref[...] = jnp.where(taken, wide_hi, 0.0).astype(jnp.bfloat16)
    lo_ref[...] = jnp.where(taken, wide_lo, 0.0).astype(jnp.bfloat16)


def mixing(member, ids, scores, sent):
    rows = ids.shape[1]
    whole = pl.BlockSpec(memory_space=pltpu.VMEM)
    return pl.pallas_call(
        mixing_kernel,
        in_specs=[pl.BlockSpec(memory_space=pltpu.SMEM)] + [whole] * 2,
        out_specs=[whole] * 2,
        out_shape=[jax.ShapeDtypeStruct((sent, rows), jnp.bfloat16)] * 2,
        compiler_params=pltpu.CompilerParams(vmem_limit_bytes=4 << 20),
        name="mixing",
    )(member.reshape(1), ids, scores)


def expert_kernel(x_ref, *refs):
    gus, downs, out_ref = refs[:GROUP], refs[GROUP : 2 * GROUP], refs[2 * GROUP]
    inner = downs[0].shape[0]
    width = out_ref.shape[1]
    hidden = []
    for gu in gus:
        both = jnp.dot(x_ref[...], gu[...], preferred_element_type=jnp.float32)
        g = jnp.minimum(both[:, :inner], clamp_limit)
        u = jnp.clip(both[:, inner:], -clamp_limit, clamp_limit)
        hidden.append(((u + 1.0) * g * jax.nn.sigmoid(swish_slope * g)).astype(jnp.bfloat16))
    hidden = jnp.concatenate(hidden, axis=1)
    step = 512
    for at in range(0, width, step):
        weights = jnp.concatenate([down[:, at : at + step] for down in downs], axis=0)
        out_ref[:, at : at + step] = jnp.dot(
            hidden, weights, preferred_element_type=jnp.float32
        ).astype(jnp.bfloat16)


def expert(x, gus, downs):
    whole = pl.BlockSpec(memory_space=pltpu.VMEM)
    return pl.pallas_call(
        expert_kernel,
        in_specs=[whole] * (1 + 2 * GROUP),
        out_specs=whole,
        out_shape=jax.ShapeDtypeStruct(x.shape, jnp.bfloat16),
        compiler_params=pltpu.CompilerParams(vmem_limit_bytes=53000 << 10),
        name="expert",
    )(x, *gus, *downs)


def program(
    mixer_in,
    mixer_gain,
    w_value,
    w_gate,
    w_taps,
    channel_gain,
    w_output,
    expert_in,
    expert_gain,
    route_experts,
    route_scores,
    expert_gate,
    expert_up,
    expert_down,
):
    rows_b, width = expert_in.shape
    experts = lax.axis_size("ep")
    capacity = 2 * rows_b * TOP_K // experts
    slots = capacity // GROUP
    member = lax.axis_index(("y0", "c")).astype(jnp.int32)

    ids = route_experts.T
    sending, gate_up = front(
        member, expert_in, expert_gain, ids, expert_gate[0], expert_up[0], experts * slots
    )
    down = expert_down[0]
    gu_y = swapped(gate_up, "y0")
    down_y = swapped(down, "y0")
    gu_c = swapped(gate_up, "c")
    down_c = swapped(down, "c")
    gu_d = swapped(gu_y, "c")
    down_d = swapped(down_y, "c")

    arrived = exchanged(sending.reshape(experts, slots, width), "ep").reshape(-1, width)

    mixing_hi, mixing_lo = mixing(member, ids, route_scores.T, experts * slots)
    conv_out = convolved(mixer_in, mixer_gain, w_value, w_gate, w_taps)
    mixer_partial = projected(conv_out, channel_gain, w_output)
    mixer_half = core_half(mixer_partial)

    partial = expert(arrived, (gate_up, gu_c, gu_y, gu_d), (down, down_c, down_y, down_d))
    returned = exchanged(partial.reshape(experts, slots, width), "ep").reshape(-1, width)

    def mixed(m):
        return lax.dot_general(
            m, returned, (((0,), (0,)), ((), ())), preferred_element_type=jnp.float32
        )

    expert_half = core_half(mixed(mixing_hi) + mixed(mixing_lo))
    mixer_out, expert_out = totals([mixer_half, expert_half])
    return (mixer_out, expert_out)


def solution(mesh):
    split = Mesh(mesh.devices.reshape(mesh.shape["ep"], 2, 2, 2, 2), ("ep", *TP))
    in_specs = (
        P("ep", None),
        P(),
        P(None, TP),
        P(None, TP),
        P(None, TP),
        P(TP),
        P(TP, None),
        P("ep", None),
        P(),
        P("ep", None),
        P("ep", None),
        P("ep", None, TP),
        P("ep", None, TP),
        P("ep", TP, None),
    )
    out_specs = (P("ep", None), P("ep", None))
    return jax.shard_map(program, mesh=split, in_specs=in_specs, out_specs=out_specs, check_vma=False)
```

```python
import jax
import jax.numpy as jnp
from jax import lax
from jax.experimental import pallas as pl
from jax.experimental.pallas import tpu as pltpu
from jax.sharding import Mesh
from jax.sharding import PartitionSpec as P

CONV_CH = 1536
CONV_W = 31
TOP_K = 4
BITS = ("y2", "y1", "y0", "c")
TP = BITS
Y = BITS[:3]
GROUP = 4
EXPERTS = 32


epsilon = 1e-05
clamp_limit = 7.0
swish_slope = 1.702


def shifted(block, axis, distance):
    devices = range(lax.axis_size(axis))
    route = [(i - distance, i) for i in devices if i - distance in devices]
    return lax.ppermute(block, axis, route)


def swapped(x, axis):
    return lax.ppermute(x, axis, [(0, 1), (1, 0)])


def exchanged(x, axis):
    return lax.all_to_all(x, axis, split_axis=0, concat_axis=0, tiled=True)


def core_half(x):
    rows, width = x.shape
    x = x.reshape(2, rows // 2, width)
    own = lax.axis_index("c")
    kept = lax.dynamic_index_in_dim(x, own, 0, keepdims=False)
    given = lax.dynamic_index_in_dim(x, 1 - own, 0, keepdims=False)
    return kept + swapped(given.astype(jnp.bfloat16), "c").astype(jnp.float32)


def totals(halves):
    size = lax.axis_size(Y)
    rows, width = halves[0].shape
    share = rows // size
    parts = [half.astype(jnp.bfloat16).reshape(size, 1, share, width) for half in halves]
    arrived = exchanged(jnp.concatenate(parts, axis=1), Y)
    summed = jnp.sum(arrived.astype(jnp.float32), axis=0).astype(jnp.bfloat16)
    gathered = exchanged(jnp.broadcast_to(summed, (size, *summed.shape)), Y)
    others = swapped(gathered, "c")
    first = lax.axis_index("c") == 0
    outs = []
    for at in range(len(halves)):
        own = gathered[:, at].reshape(rows, width)
        other = others[:, at].reshape(rows, width)
        low, high = jnp.where(first, own, other), jnp.where(first, other, own)
        outs.append(jnp.concatenate([low, high], axis=0))
    return outs


def row_norm(inputs, gains):
    widened = inputs.astype(jnp.float32)
    row_mean = jnp.mean(widened, axis=-1, keepdims=True)
    row_var = jnp.mean(jnp.square(widened - row_mean), axis=-1, keepdims=True)
    return (widened - row_mean) * lax.rsqrt(row_var + epsilon) * gains


def convolved(mixer_in, mixer_gain, w_value, w_gate, w_taps):
    normed = row_norm(mixer_in, mixer_gain).astype(jnp.bfloat16)
    values = jnp.dot(normed, w_value, preferred_element_type=jnp.float32)
    gate_pre = jnp.dot(normed, w_gate, preferred_element_type=jnp.float32)
    gated_values = (values * jax.nn.sigmoid(gate_pre)).astype(jnp.bfloat16)
    mixer_rows = gated_values.shape[0]
    reach_rows = CONV_W - 1
    earlier = shifted(gated_values[mixer_rows - reach_rows :], "ep", 1)
    extended = jnp.concatenate([earlier, gated_values], axis=0)
    conv_out = jnp.zeros(gated_values.shape, jnp.float32)
    for offset in range(CONV_W):
        conv_out = (
            conv_out + extended[offset : offset + mixer_rows].astype(jnp.float32) * w_taps[offset]
        )
    return conv_out


def projected(conv_out, channel_gain, w_output):
    sums = jnp.stack([jnp.sum(conv_out, axis=1), jnp.sum(conv_out * conv_out, axis=1)])
    everyone = lax.all_gather(sums, TP)
    sums = jnp.sum(everyone, axis=0)
    row_mean = (sums[0] / CONV_CH)[:, None]
    row_var = (sums[1] / CONV_CH)[:, None] - row_mean * row_mean
    activated = jax.nn.silu(
        (conv_out - row_mean) * lax.rsqrt(row_var + epsilon) * channel_gain
    ).astype(jnp.bfloat16)
    return jnp.dot(activated, w_output, preferred_element_type=jnp.float32)


def places(ids_ref, rows):
    names = lax.broadcasted_iota(jnp.int32, (EXPERTS, rows), 0)
    named = [ids_ref[pl.ds(k, 1), :] == names for k in range(TOP_K)]
    chosen = jnp.zeros((EXPERTS, rows), jnp.float32)
    for k in range(TOP_K):
        chosen = jnp.where(named[k], 1.0, chosen)
    earlier = lax.broadcasted_iota(jnp.int32, (rows, rows), 0)
    later = lax.broadcasted_iota(jnp.int32, (rows, rows), 1)
    before = jnp.where(earlier < later, 1.0, 0.0).astype(jnp.bfloat16)
    rank = jnp.dot(chosen.astype(jnp.bfloat16), before, preferred_element_type=jnp.float32)
    return named, jnp.where(chosen > 0.0, rank, -1.0).astype(jnp.bfloat16)


def spread_over(sent, per_expert):
    of_row = lax.broadcasted_iota(jnp.int32, (sent, EXPERTS), 0) // per_expert
    of_col = lax.broadcasted_iota(jnp.int32, (sent, EXPERTS), 1)
    return jnp.where(of_row == of_col, 1.0, 0.0).astype(jnp.bfloat16)


def taken_by(place, spread, slots, member):
    sent, rows = spread.shape[0], place.shape[1]
    slot = lax.broadcasted_iota(jnp.int32, (sent, rows), 0) % slots * GROUP + member
    return jnp.dot(spread, place, preferred_element_type=jnp.float32) == slot.astype(jnp.float32)


def front_kernel(member, x_ref, gain_ref, ids_ref, rows_ref):
    rows = x_ref.shape[0]
    sent = rows_ref.shape[0]
    slots = sent // EXPERTS
    normed = row_norm(x_ref[...], gain_ref[...]).astype(jnp.bfloat16)
    _, place = places(ids_ref, rows)
    taken = taken_by(place, spread_over(sent, slots), slots, member[0])
    select = jnp.where(taken, 1.0, 0.0).astype(jnp.bfloat16)
    rows_ref[...] = jnp.dot(select, normed, preferred_element_type=jnp.float32).astype(jnp.bfloat16)


def front(member, x, gain, ids, sent):
    _, width = x.shape
    whole = pl.BlockSpec(memory_space=pltpu.VMEM)
    return pl.pallas_call(
        front_kernel,
        in_specs=[pl.BlockSpec(memory_space=pltpu.SMEM)] + [whole] * 3,
        out_specs=whole,
        out_shape=jax.ShapeDtypeStruct((sent, width), jnp.bfloat16),
        compiler_params=pltpu.CompilerParams(vmem_limit_bytes=8 << 20),
        name="front",
    )(member.reshape(1), x, gain.reshape(1, width), ids)


def mixing_kernel(member, ids_ref, scores_ref, hi_ref, lo_ref):
    sent, rows = hi_ref.shape
    slots = sent // EXPERTS
    raised = [jnp.exp(scores_ref[pl.ds(k, 1), :]) for k in range(TOP_K)]
    total = raised[0] + raised[1] + raised[2] + raised[3]
    named, place = places(ids_ref, rows)
    weights = jnp.zeros((EXPERTS, rows), jnp.float32)
    for k in range(TOP_K):
        weights = jnp.where(named[k], raised[k] / total, weights)
    weights_hi = weights.astype(jnp.bfloat16)
    weights_lo = (weights - weights_hi.astype(jnp.float32)).astype(jnp.bfloat16)
    spread = spread_over(sent, slots)
    taken = taken_by(place, spread, slots, member[0])
    wide_hi = jnp.dot(spread, weights_hi, preferred_element_type=jnp.float32)
    wide_lo = jnp.dot(spread, weights_lo, preferred_element_type=jnp.float32)
    hi_ref[...] = jnp.where(taken, wide_hi, 0.0).astype(jnp.bfloat16)
    lo_ref[...] = jnp.where(taken, wide_lo, 0.0).astype(jnp.bfloat16)


def mixing(member, ids, scores, sent):
    rows = ids.shape[1]
    whole = pl.BlockSpec(memory_space=pltpu.VMEM)
    return pl.pallas_call(
        mixing_kernel,
        in_specs=[pl.BlockSpec(memory_space=pltpu.SMEM)] + [whole] * 2,
        out_specs=[whole] * 2,
        out_shape=[jax.ShapeDtypeStruct((sent, rows), jnp.bfloat16)] * 2,
        compiler_params=pltpu.CompilerParams(vmem_limit_bytes=4 << 20),
        name="mixing",
    )(member.reshape(1), ids, scores)


def hidden_kernel(x_ref, *refs):
    gus, out_ref = refs[:GROUP], refs[GROUP]
    inner = gus[0].shape[1] // 2
    for at, gu in enumerate(gus):
        both = jnp.dot(x_ref[...], gu[...], preferred_element_type=jnp.float32)
        g = jnp.minimum(both[:, :inner], clamp_limit)
        u = jnp.clip(both[:, inner:], -clamp_limit, clamp_limit)
        hidden = (u + 1.0) * g * jax.nn.sigmoid(swish_slope * g)
        out_ref[:, at * inner : (at + 1) * inner] = hidden.astype(jnp.bfloat16)


def down_kernel(hidden_ref, *refs):
    downs, out_ref = refs[:GROUP], refs[GROUP]
    step = 512
    for at in range(0, out_ref.shape[1], step):
        weights = jnp.concatenate([down[:, at : at + step] for down in downs], axis=0)
        out_ref[:, at : at + step] = jnp.dot(
            hidden_ref[...], weights, preferred_element_type=jnp.float32
        ).astype(jnp.bfloat16)


def in_vmem(kernel, limit, shape, *operands):
    whole = pl.BlockSpec(memory_space=pltpu.VMEM)
    return pl.pallas_call(
        kernel,
        in_specs=[whole] * len(operands),
        out_specs=whole,
        out_shape=jax.ShapeDtypeStruct(shape, jnp.bfloat16),
        compiler_params=pltpu.CompilerParams(vmem_limit_bytes=limit << 10),
    )(*operands)


def program(
    mixer_in,
    mixer_gain,
    w_value,
    w_gate,
    w_taps,
    channel_gain,
    w_output,
    expert_in,
    expert_gain,
    route_experts,
    route_scores,
    expert_gate,
    expert_up,
    expert_down,
):
    rows_b, width = expert_in.shape
    experts = lax.axis_size("ep")
    capacity = 2 * rows_b * TOP_K // experts
    slots = capacity // GROUP
    member = lax.axis_index(("y0", "c")).astype(jnp.int32)

    gate_up = jnp.concatenate([expert_gate[0], expert_up[0]], axis=1)
    down = expert_down[0]
    gu_y = swapped(gate_up, "y0")
    down_y = swapped(down, "y0")
    gu_c = swapped(gate_up, "c")
    down_c = swapped(down, "c")
    gu_d = swapped(gu_y, "c")
    down_d = swapped(down_y, "c")

    ids = route_experts.T
    sending = front(member, expert_in, expert_gain, ids, experts * slots)
    arrived = exchanged(sending.reshape(experts, slots, width), "ep").reshape(-1, width)

    mixing_hi, mixing_lo = mixing(member, ids, route_scores.T, experts * slots)
    conv_out = convolved(mixer_in, mixer_gain, w_value, w_gate, w_taps)
    mixer_partial = projected(conv_out, channel_gain, w_output)
    mixer_half = core_half(mixer_partial)

    hidden_shape = (experts * slots, GROUP * down.shape[0])
    hidden = in_vmem(hidden_kernel, 53000, hidden_shape, arrived, gate_up, gu_c, gu_y, gu_d)
    partial = in_vmem(down_kernel, 53000, arrived.shape, hidden, down, down_c, down_y, down_d)
    returned = exchanged(partial.reshape(experts, slots, width), "ep").reshape(-1, width)

    def mixed(m):
        return lax.dot_general(
            m, returned, (((0,), (0,)), ((), ())), preferred_element_type=jnp.float32
        )

    expert_half = core_half(mixed(mixing_hi) + mixed(mixing_lo))
    mixer_out, expert_out = totals([mixer_half, expert_half])
    return (mixer_out, expert_out)


def solution(mesh):
    split = Mesh(mesh.devices.reshape(mesh.shape["ep"], 2, 2, 2, 2), ("ep", *TP))
    in_specs = (
        P("ep", None),
        P(),
        P(None, TP),
        P(None, TP),
        P(None, TP),
        P(TP),
        P(TP, None),
        P("ep", None),
        P(),
        P("ep", None),
        P("ep", None),
        P("ep", None, TP),
        P("ep", None, TP),
        P("ep", TP, None),
    )
    out_specs = (P("ep", None), P("ep", None))
    return jax.shard_map(program, mesh=split, in_specs=in_specs, out_specs=out_specs, check_vma=False)
```

```python
import jax
import jax.numpy as jnp
from jax import lax
from jax.experimental import pallas as pl
from jax.experimental.pallas import tpu as pltpu
from jax.sharding import Mesh
from jax.sharding import PartitionSpec as P

CONV_CH = 1536
CONV_W = 31
TOP_K = 4
BITS = ("y2", "y1", "y0", "c")
TP = BITS
Y = BITS[:3]
GROUP = 4
EXPERTS = 32


epsilon = 1e-05
clamp_limit = 7.0
swish_slope = 1.702


def shifted(block, axis, distance):
    devices = range(lax.axis_size(axis))
    route = [(i - distance, i) for i in devices if i - distance in devices]
    return lax.ppermute(block, axis, route)


def swapped(x, axis):
    return lax.ppermute(x, axis, [(0, 1), (1, 0)])


def exchanged(x, axis):
    return lax.all_to_all(x, axis, split_axis=0, concat_axis=0, tiled=True)


def core_half(x):
    rows, width = x.shape
    x = x.reshape(2, rows // 2, width)
    own = lax.axis_index("c")
    kept = lax.dynamic_index_in_dim(x, own, 0, keepdims=False)
    given = lax.dynamic_index_in_dim(x, 1 - own, 0, keepdims=False)
    return kept + swapped(given.astype(jnp.bfloat16), "c").astype(jnp.float32)


def totals(halves):
    size = lax.axis_size(Y)
    rows, width = halves[0].shape
    share = rows // size
    parts = [half.astype(jnp.bfloat16).reshape(size, 1, share, width) for half in halves]
    arrived = exchanged(jnp.concatenate(parts, axis=1), Y)
    summed = jnp.sum(arrived.astype(jnp.float32), axis=0).astype(jnp.bfloat16)
    gathered = exchanged(jnp.broadcast_to(summed, (size, *summed.shape)), Y)
    others = swapped(gathered, "c")
    first = lax.axis_index("c") == 0
    outs = []
    for at in range(len(halves)):
        own = gathered[:, at].reshape(rows, width)
        other = others[:, at].reshape(rows, width)
        low, high = jnp.where(first, own, other), jnp.where(first, other, own)
        outs.append(jnp.concatenate([low, high], axis=0))
    return outs


def row_norm(inputs, gains):
    widened = inputs.astype(jnp.float32)
    row_mean = jnp.mean(widened, axis=-1, keepdims=True)
    row_var = jnp.mean(jnp.square(widened - row_mean), axis=-1, keepdims=True)
    return (widened - row_mean) * lax.rsqrt(row_var + epsilon) * gains


def convolved(mixer_in, mixer_gain, w_value, w_gate, w_taps):
    normed = row_norm(mixer_in, mixer_gain).astype(jnp.bfloat16)
    values = jnp.dot(normed, w_value, preferred_element_type=jnp.float32)
    gate_pre = jnp.dot(normed, w_gate, preferred_element_type=jnp.float32)
    gated_values = (values * jax.nn.sigmoid(gate_pre)).astype(jnp.bfloat16)
    mixer_rows = gated_values.shape[0]
    reach_rows = CONV_W - 1
    earlier = shifted(gated_values[mixer_rows - reach_rows :], "ep", 1)
    extended = jnp.concatenate([earlier, gated_values], axis=0)
    conv_out = jnp.zeros(gated_values.shape, jnp.float32)
    for offset in range(CONV_W):
        conv_out = (
            conv_out + extended[offset : offset + mixer_rows].astype(jnp.float32) * w_taps[offset]
        )
    return conv_out


def projected(conv_out, channel_gain, w_output):
    sums = jnp.stack([jnp.sum(conv_out, axis=1), jnp.sum(conv_out * conv_out, axis=1)])
    everyone = lax.all_gather(sums, TP)
    sums = jnp.sum(everyone, axis=0)
    row_mean = (sums[0] / CONV_CH)[:, None]
    row_var = (sums[1] / CONV_CH)[:, None] - row_mean * row_mean
    activated = jax.nn.silu(
        (conv_out - row_mean) * lax.rsqrt(row_var + epsilon) * channel_gain
    ).astype(jnp.bfloat16)
    return jnp.dot(activated, w_output, preferred_element_type=jnp.float32)


def places(ids_ref, rows):
    names = lax.broadcasted_iota(jnp.int32, (EXPERTS, rows), 0)
    named = [ids_ref[pl.ds(k, 1), :] == names for k in range(TOP_K)]
    chosen = jnp.zeros((EXPERTS, rows), jnp.float32)
    for k in range(TOP_K):
        chosen = jnp.where(named[k], 1.0, chosen)
    earlier = lax.broadcasted_iota(jnp.int32, (rows, rows), 0)
    later = lax.broadcasted_iota(jnp.int32, (rows, rows), 1)
    before = jnp.where(earlier < later, 1.0, 0.0).astype(jnp.bfloat16)
    rank = jnp.dot(chosen.astype(jnp.bfloat16), before, preferred_element_type=jnp.float32)
    return named, jnp.where(chosen > 0.0, rank, -1.0).astype(jnp.bfloat16)


def spread_over(sent, per_expert):
    of_row = lax.broadcasted_iota(jnp.int32, (sent, EXPERTS), 0) // per_expert
    of_col = lax.broadcasted_iota(jnp.int32, (sent, EXPERTS), 1)
    return jnp.where(of_row == of_col, 1.0, 0.0).astype(jnp.bfloat16)


def taken_by(place, spread, slots, member):
    sent, rows = spread.shape[0], place.shape[1]
    slot = lax.broadcasted_iota(jnp.int32, (sent, rows), 0) % slots * GROUP + member
    return jnp.dot(spread, place, preferred_element_type=jnp.float32) == slot.astype(jnp.float32)


def front_kernel(member, x_ref, gain_ref, ids_ref, rows_ref):
    rows = x_ref.shape[0]
    sent = rows_ref.shape[0]
    slots = sent // EXPERTS
    normed = row_norm(x_ref[...], gain_ref[...]).astype(jnp.bfloat16)
    _, place = places(ids_ref, rows)
    taken = taken_by(place, spread_over(sent, slots), slots, member[0])
    select = jnp.where(taken, 1.0, 0.0).astype(jnp.bfloat16)
    rows_ref[...] = jnp.dot(select, normed, preferred_element_type=jnp.float32).astype(jnp.bfloat16)


def front(member, x, gain, ids, sent):
    _, width = x.shape
    whole = pl.BlockSpec(memory_space=pltpu.VMEM)
    return pl.pallas_call(
        front_kernel,
        in_specs=[pl.BlockSpec(memory_space=pltpu.SMEM)] + [whole] * 3,
        out_specs=whole,
        out_shape=jax.ShapeDtypeStruct((sent, width), jnp.bfloat16),
        compiler_params=pltpu.CompilerParams(vmem_limit_bytes=60 * 1024 * 1024),
        name="front",
    )(member.reshape(1), x, gain.reshape(1, width), ids)


def mixing_kernel(member, ids_ref, scores_ref, hi_ref, lo_ref):
    sent, rows = hi_ref.shape
    slots = sent // EXPERTS
    raised = [jnp.exp(scores_ref[pl.ds(k, 1), :]) for k in range(TOP_K)]
    total = raised[0] + raised[1] + raised[2] + raised[3]
    named, place = places(ids_ref, rows)
    weights = jnp.zeros((EXPERTS, rows), jnp.float32)
    for k in range(TOP_K):
        weights = jnp.where(named[k], raised[k] / total, weights)
    weights_hi = weights.astype(jnp.bfloat16)
    weights_lo = (weights - weights_hi.astype(jnp.float32)).astype(jnp.bfloat16)
    spread = spread_over(sent, slots)
    taken = taken_by(place, spread, slots, member[0])
    wide_hi = jnp.dot(spread, weights_hi, preferred_element_type=jnp.float32)
    wide_lo = jnp.dot(spread, weights_lo, preferred_element_type=jnp.float32)
    hi_ref[...] = jnp.where(taken, wide_hi, 0.0).astype(jnp.bfloat16)
    lo_ref[...] = jnp.where(taken, wide_lo, 0.0).astype(jnp.bfloat16)


def mixing(member, ids, scores, sent):
    rows = ids.shape[1]
    whole = pl.BlockSpec(memory_space=pltpu.VMEM)
    return pl.pallas_call(
        mixing_kernel,
        in_specs=[pl.BlockSpec(memory_space=pltpu.SMEM)] + [whole] * 2,
        out_specs=[whole] * 2,
        out_shape=[jax.ShapeDtypeStruct((sent, rows), jnp.bfloat16)] * 2,
        compiler_params=pltpu.CompilerParams(vmem_limit_bytes=4 << 20),
        name="mixing",
    )(member.reshape(1), ids, scores)


def hidden_kernel(x_ref, *refs):
    gates, ups, out_ref = refs[:GROUP], refs[GROUP : 2 * GROUP], refs[2 * GROUP]
    inner = gates[0].shape[1]
    for at, (gate, up) in enumerate(zip(gates, ups, strict=True)):
        weights = jnp.concatenate([gate[...], up[...]], axis=1)
        both = jnp.dot(x_ref[...], weights, preferred_element_type=jnp.float32)
        g = jnp.minimum(both[:, :inner], clamp_limit)
        u = jnp.clip(both[:, inner:], -clamp_limit, clamp_limit)
        hidden = (u + 1.0) * g * jax.nn.sigmoid(swish_slope * g)
        out_ref[:, at * inner : (at + 1) * inner] = hidden.astype(jnp.bfloat16)


def down_kernel(hidden_ref, *refs):
    downs, out_ref = refs[:GROUP], refs[GROUP]
    step = 512
    for at in range(0, out_ref.shape[1], step):
        weights = jnp.concatenate([down[:, at : at + step] for down in downs], axis=0)
        out_ref[:, at : at + step] = jnp.dot(
            hidden_ref[...], weights, preferred_element_type=jnp.float32
        ).astype(jnp.bfloat16)


def in_vmem(kernel, limit, shape, *operands):
    whole = pl.BlockSpec(memory_space=pltpu.VMEM)
    return pl.pallas_call(
        kernel,
        in_specs=[whole] * len(operands),
        out_specs=whole,
        out_shape=jax.ShapeDtypeStruct(shape, jnp.bfloat16),
        compiler_params=pltpu.CompilerParams(vmem_limit_bytes=limit << 10),
    )(*operands)


def program(
    mixer_in,
    mixer_gain,
    w_value,
    w_gate,
    w_taps,
    channel_gain,
    w_output,
    expert_in,
    expert_gain,
    route_experts,
    route_scores,
    expert_gate,
    expert_up,
    expert_down,
):
    rows_b, width = expert_in.shape
    experts = lax.axis_size("ep")
    capacity = 2 * rows_b * TOP_K // experts
    slots = capacity // GROUP
    member = lax.axis_index(("y0", "c")).astype(jnp.int32)

    own = {"gate": expert_gate[0], "up": expert_up[0], "down": expert_down[0]}
    weights = {name: [w] for name, w in own.items()}
    for name, w in own.items():
        weights[name].append(swapped(w, "c"))
        near = swapped(w, "y0")
        weights[name] += [near, swapped(near, "c")]

    ids = route_experts.T
    sending = front(member, expert_in, expert_gain, ids, experts * slots)
    arrived = exchanged(sending.reshape(experts, slots, width), "ep").reshape(-1, width)

    mixing_hi, mixing_lo = mixing(member, ids, route_scores.T, experts * slots)
    conv_out = convolved(mixer_in, mixer_gain, w_value, w_gate, w_taps)
    mixer_partial = projected(conv_out, channel_gain, w_output)
    mixer_half = core_half(mixer_partial)

    hidden_shape = (experts * slots, GROUP * own["down"].shape[0])
    pairs = (arrived, *weights["gate"], *weights["up"])
    hidden = in_vmem(hidden_kernel, 53000, hidden_shape, *pairs)
    partial = in_vmem(down_kernel, 53000, arrived.shape, hidden, *weights["down"])
    returned = exchanged(partial.reshape(experts, slots, width), "ep").reshape(-1, width)

    def mixed(m):
        return lax.dot_general(
            m, returned, (((0,), (0,)), ((), ())), preferred_element_type=jnp.float32
        )

    expert_half = core_half(mixed(mixing_hi) + mixed(mixing_lo))
    mixer_out, expert_out = totals([mixer_half, expert_half])
    return (mixer_out, expert_out)


def solution(mesh):
    split = Mesh(mesh.devices.reshape(mesh.shape["ep"], 2, 2, 2, 2), ("ep", *TP))
    in_specs = (
        P("ep", None),
        P(),
        P(None, TP),
        P(None, TP),
        P(None, TP),
        P(TP),
        P(TP, None),
        P("ep", None),
        P(),
        P("ep", None),
        P("ep", None),
        P("ep", None, TP),
        P("ep", None, TP),
        P("ep", TP, None),
    )
    out_specs = (P("ep", None), P("ep", None))
    return jax.shard_map(program, mesh=split, in_specs=in_specs, out_specs=out_specs, check_vma=False)
```

```python
import jax
import jax.numpy as jnp
from jax import lax
from jax.experimental import pallas as pl
from jax.experimental.pallas import tpu as pltpu
from jax.sharding import Mesh
from jax.sharding import PartitionSpec as P

CONV_CH = 1536
CONV_W = 31
TOP_K = 4
BITS = ("y2", "y1", "y0", "c")
TP = BITS
Y = BITS[:3]
GROUP = 4
EXPERTS = 32


epsilon = 1e-05
clamp_limit = 7.0
swish_slope = 1.702


def shifted(block, axis, distance):
    devices = range(lax.axis_size(axis))
    route = [(i - distance, i) for i in devices if i - distance in devices]
    return lax.ppermute(block, axis, route)


def swapped(x, axis):
    return lax.ppermute(x, axis, [(0, 1), (1, 0)])


def exchanged(x, axis):
    return lax.all_to_all(x, axis, split_axis=0, concat_axis=0, tiled=True)


def core_half(x):
    rows, width = x.shape
    x = x.reshape(2, rows // 2, width)
    own = lax.axis_index("c")
    kept = lax.dynamic_index_in_dim(x, own, 0, keepdims=False)
    given = lax.dynamic_index_in_dim(x, 1 - own, 0, keepdims=False)
    return kept + swapped(given.astype(jnp.bfloat16), "c").astype(jnp.float32)


def totals(halves):
    size = lax.axis_size(Y)
    rows, width = halves[0].shape
    share = rows // size
    parts = [half.astype(jnp.bfloat16).reshape(size, 1, share, width) for half in halves]
    arrived = exchanged(jnp.concatenate(parts, axis=1), Y)
    summed = jnp.sum(arrived.astype(jnp.float32), axis=0).astype(jnp.bfloat16)
    gathered = exchanged(jnp.broadcast_to(summed, (size, *summed.shape)), Y)
    others = swapped(gathered, "c")
    return placed(gathered, others)


def row_norm(inputs, gains):
    widened = inputs.astype(jnp.float32)
    row_mean = jnp.mean(widened, axis=-1, keepdims=True)
    row_var = jnp.mean(jnp.square(widened - row_mean), axis=-1, keepdims=True)
    return (widened - row_mean) * lax.rsqrt(row_var + epsilon) * gains


def gating_kernel(x_ref, gain_ref, value_ref, gate_ref, out_ref, last_ref):
    normed = row_norm(x_ref[...], gain_ref[...]).astype(jnp.bfloat16)
    across = (((1,), (1,)), ((), ()))
    values, gates = (
        lax.dot_general(w[...], normed, across, preferred_element_type=jnp.float32)
        for w in (value_ref, gate_ref)
    )
    gated = (values * jax.nn.sigmoid(gates)).astype(jnp.bfloat16)
    out_ref[...] = gated
    last_ref[...] = gated[:, gated.shape[1] - last_ref.shape[1] :]


def gated_channels(x, gain, w_value, w_gate):
    rows, width = x.shape
    channels = w_value.shape[1]
    return pl.pallas_call(
        gating_kernel,
        in_specs=[WHOLE] * 4,
        out_specs=[WHOLE] * 2,
        out_shape=[
            jax.ShapeDtypeStruct((channels, rows), jnp.bfloat16),
            jax.ShapeDtypeStruct((channels, CONV_W - 1), jnp.bfloat16),
        ],
        compiler_params=pltpu.CompilerParams(vmem_limit_bytes=8 << 20),
        name="gating",
    )(x, gain.reshape(1, width), w_value.T, w_gate.T)


def convolved(gated_values, last_rows, w_taps):
    rows = gated_values.shape[1]
    earlier = shifted(last_rows, "ep", 1)
    extended = jnp.concatenate([earlier, gated_values], axis=1)
    conv_out = jnp.zeros(gated_values.shape, jnp.float32)
    for offset in range(CONV_W):
        taps = w_taps[offset][:, None]
        conv_out = conv_out + extended[:, offset : offset + rows].astype(jnp.float32) * taps
    return conv_out


def projected(conv_out, channel_gain, w_output):
    sums = jnp.stack([jnp.sum(conv_out, axis=0), jnp.sum(conv_out * conv_out, axis=0)])
    everyone = lax.all_gather(sums, TP)
    sums = jnp.sum(everyone, axis=0)
    row_mean = (sums[0] / CONV_CH)[None, :]
    row_var = (sums[1] / CONV_CH)[None, :] - row_mean * row_mean
    activated = jax.nn.silu(
        (conv_out - row_mean) * lax.rsqrt(row_var + epsilon) * channel_gain[:, None]
    ).astype(jnp.bfloat16)
    return lax.dot_general(
        activated, w_output, (((0,), (0,)), ((), ())), preferred_element_type=jnp.float32
    )


def places(ids_ref, rows):
    names = lax.broadcasted_iota(jnp.int32, (EXPERTS, rows), 0)
    named = [ids_ref[pl.ds(k, 1), :] == names for k in range(TOP_K)]
    chosen = jnp.zeros((EXPERTS, rows), jnp.float32)
    for k in range(TOP_K):
        chosen = jnp.where(named[k], 1.0, chosen)
    earlier = lax.broadcasted_iota(jnp.int32, (rows, rows), 0)
    later = lax.broadcasted_iota(jnp.int32, (rows, rows), 1)
    before = jnp.where(earlier < later, 1.0, 0.0).astype(jnp.bfloat16)
    rank = jnp.dot(chosen.astype(jnp.bfloat16), before, preferred_element_type=jnp.float32)
    return named, jnp.where(chosen > 0.0, rank, -1.0).astype(jnp.bfloat16)


def spread_over(sent, per_expert):
    of_row = lax.broadcasted_iota(jnp.int32, (sent, EXPERTS), 0) // per_expert
    of_col = lax.broadcasted_iota(jnp.int32, (sent, EXPERTS), 1)
    return jnp.where(of_row == of_col, 1.0, 0.0).astype(jnp.bfloat16)


def taken_by(place, spread, slots, member):
    sent, rows = spread.shape[0], place.shape[1]
    slot = lax.broadcasted_iota(jnp.int32, (sent, rows), 0) % slots * GROUP + member
    return jnp.dot(spread, place, preferred_element_type=jnp.float32) == slot.astype(jnp.float32)


def front_kernel(member, x_ref, gain_ref, ids_ref, rows_ref):
    rows = x_ref.shape[0]
    sent = rows_ref.shape[0]
    slots = sent // EXPERTS
    normed = row_norm(x_ref[...], gain_ref[...]).astype(jnp.bfloat16)
    _, place = places(ids_ref, rows)
    taken = taken_by(place, spread_over(sent, slots), slots, member[0])
    select = jnp.where(taken, 1.0, 0.0).astype(jnp.bfloat16)
    rows_ref[...] = jnp.dot(select, normed, preferred_element_type=jnp.float32).astype(jnp.bfloat16)


def front(member, x, gain, ids, sent):
    _, width = x.shape
    whole = pl.BlockSpec(memory_space=pltpu.VMEM)
    return pl.pallas_call(
        front_kernel,
        in_specs=[pl.BlockSpec(memory_space=pltpu.SMEM)] + [whole] * 3,
        out_specs=whole,
        out_shape=jax.ShapeDtypeStruct((sent, width), jnp.bfloat16),
        compiler_params=pltpu.CompilerParams(vmem_limit_bytes=60 * 1024 * 1024),
        name="front",
    )(member.reshape(1), x, gain.reshape(1, width), ids)


def mixing_kernel(member, ids_ref, scores_ref, hi_ref, lo_ref):
    sent, rows = hi_ref.shape
    slots = sent // EXPERTS
    raised = [jnp.exp(scores_ref[pl.ds(k, 1), :]) for k in range(TOP_K)]
    total = raised[0] + raised[1] + raised[2] + raised[3]
    named, place = places(ids_ref, rows)
    weights = jnp.zeros((EXPERTS, rows), jnp.float32)
    for k in range(TOP_K):
        weights = jnp.where(named[k], raised[k] / total, weights)
    weights_hi = weights.astype(jnp.bfloat16)
    weights_lo = (weights - weights_hi.astype(jnp.float32)).astype(jnp.bfloat16)
    spread = spread_over(sent, slots)
    taken = taken_by(place, spread, slots, member[0])
    wide_hi = jnp.dot(spread, weights_hi, preferred_element_type=jnp.float32)
    wide_lo = jnp.dot(spread, weights_lo, preferred_element_type=jnp.float32)
    hi_ref[...] = jnp.where(taken, wide_hi, 0.0).astype(jnp.bfloat16)
    lo_ref[...] = jnp.where(taken, wide_lo, 0.0).astype(jnp.bfloat16)


def mixing(member, ids, scores, sent):
    rows = ids.shape[1]
    whole = pl.BlockSpec(memory_space=pltpu.VMEM)
    return pl.pallas_call(
        mixing_kernel,
        in_specs=[pl.BlockSpec(memory_space=pltpu.SMEM)] + [whole] * 2,
        out_specs=[whole] * 2,
        out_shape=[jax.ShapeDtypeStruct((sent, rows), jnp.bfloat16)] * 2,
        compiler_params=pltpu.CompilerParams(vmem_limit_bytes=4 << 20),
        name="mixing",
    )(member.reshape(1), ids, scores)


def hidden_kernel(x_ref, *refs):
    gates, ups, out_ref = refs[:GROUP], refs[GROUP : 2 * GROUP], refs[2 * GROUP]
    inner = gates[0].shape[1]
    for at, (gate, up) in enumerate(zip(gates, ups, strict=True)):
        weights = jnp.concatenate([gate[...], up[...]], axis=1)
        both = jnp.dot(x_ref[...], weights, preferred_element_type=jnp.float32)
        g = jnp.minimum(both[:, :inner], clamp_limit)
        u = jnp.clip(both[:, inner:], -clamp_limit, clamp_limit)
        hidden = (u + 1.0) * g * jax.nn.sigmoid(swish_slope * g)
        out_ref[:, at * inner : (at + 1) * inner] = hidden.astype(jnp.bfloat16)


def down_kernel(hidden_ref, *refs):
    downs, out_hbm, out_buf, sems = refs[:GROUP], refs[GROUP], refs[GROUP + 1], refs[GROUP + 2]
    parts = sems.shape[0]
    step = out_hbm.shape[1] // parts
    copies = []
    for part in range(parts):
        own = pl.ds(part * step, step)
        weights = jnp.concatenate([down[:, own] for down in downs], axis=0)
        out_buf[:, own] = jnp.dot(
            hidden_ref[...], weights, preferred_element_type=jnp.float32
        ).astype(jnp.bfloat16)
        copies.append(pltpu.make_async_copy(out_buf.at[:, own], out_hbm.at[:, own], sems.at[part]))
        copies[-1].start()
    for copy in copies:
        copy.wait()


WHOLE = pl.BlockSpec(memory_space=pltpu.VMEM)
OUTSIDE = pl.BlockSpec(memory_space=pl.ANY)


def hidden_units(x, gates, ups):
    units = GROUP * gates[0].shape[1]
    return pl.pallas_call(
        hidden_kernel,
        in_specs=[WHOLE] * (1 + 2 * GROUP),
        out_specs=WHOLE,
        out_shape=jax.ShapeDtypeStruct((x.shape[0], units), jnp.bfloat16),
        compiler_params=pltpu.CompilerParams(vmem_limit_bytes=53000 << 10),
        name="hidden",
    )(x, *gates, *ups)


def projected_down(hidden, downs):
    shape = (hidden.shape[0], downs[0].shape[1])
    return pl.pallas_call(
        down_kernel,
        in_specs=[WHOLE] * (1 + GROUP),
        out_specs=OUTSIDE,
        out_shape=jax.ShapeDtypeStruct(shape, jnp.bfloat16),
        scratch_shapes=[pltpu.VMEM(shape, jnp.bfloat16), pltpu.SemaphoreType.DMA((4,))],
        compiler_params=pltpu.CompilerParams(vmem_limit_bytes=53000 << 10),
        name="project",
    )(hidden, *downs)


def placing_kernel(core, own_ref, other_ref, *refs):
    outs, sems = refs[:-1], refs[-1]
    copies = []
    for at, out in enumerate(outs):
        for side, ref in enumerate((own_ref, other_ref)):
            place = core[0] if side == 0 else 1 - core[0]
            copies.append(pltpu.make_async_copy(ref.at[:, at], out.at[place], sems.at[at, side]))
            copies[-1].start()
    for copy in copies:
        copy.wait()


def placed(own, other):
    blocks, count, rows, width = own.shape
    core = lax.axis_index("c").astype(jnp.int32).reshape(1)
    outs = pl.pallas_call(
        placing_kernel,
        in_specs=[pl.BlockSpec(memory_space=pltpu.SMEM), OUTSIDE, OUTSIDE],
        out_specs=[OUTSIDE] * count,
        out_shape=[jax.ShapeDtypeStruct((2, blocks, rows, width), own.dtype)] * count,
        scratch_shapes=[pltpu.SemaphoreType.DMA((count, 2))],
        compiler_params=pltpu.CompilerParams(vmem_limit_bytes=1 << 20),
        name="placing",
    )(core, own, other)
    return [out.reshape(2 * blocks * rows, width) for out in outs]


def program(
    mixer_in,
    mixer_gain,
    w_value,
    w_gate,
    w_taps,
    channel_gain,
    w_output,
    expert_in,
    expert_gain,
    route_experts,
    route_scores,
    expert_gate,
    expert_up,
    expert_down,
):
    rows_b, width = expert_in.shape
    experts = lax.axis_size("ep")
    capacity = 2 * rows_b * TOP_K // experts
    slots = capacity // GROUP
    member = lax.axis_index(("y0", "c")).astype(jnp.int32)

    own = {"gate": expert_gate[0], "up": expert_up[0], "down": expert_down[0]}
    weights = {name: [w] for name, w in own.items()}
    for name, w in own.items():
        weights[name].append(swapped(w, "c"))
        near = swapped(w, "y0")
        weights[name] += [near, swapped(near, "c")]

    ids = route_experts.T
    sending = front(member, expert_in, expert_gain, ids, experts * slots)
    arrived = exchanged(sending.reshape(experts, slots, width), "ep").reshape(-1, width)

    mixing_hi, mixing_lo = mixing(member, ids, route_scores.T, experts * slots)
    conv_out = convolved(*gated_channels(mixer_in, mixer_gain, w_value, w_gate), w_taps)
    mixer_partial = projected(conv_out, channel_gain, w_output)
    mixer_half = core_half(mixer_partial)

    hidden = hidden_units(arrived, weights["gate"], weights["up"])
    partial = projected_down(hidden, weights["down"])
    returned = exchanged(partial.reshape(experts, slots, width), "ep").reshape(-1, width)

    def mixed(m):
        return lax.dot_general(
            m, returned, (((0,), (0,)), ((), ())), preferred_element_type=jnp.float32
        )

    expert_half = core_half(mixed(mixing_hi) + mixed(mixing_lo))
    mixer_out, expert_out = totals([mixer_half, expert_half])
    return (mixer_out, expert_out)


def solution(mesh):
    split = Mesh(mesh.devices.reshape(mesh.shape["ep"], 2, 2, 2, 2), ("ep", *TP))
    in_specs = (
        P("ep", None),
        P(),
        P(None, TP),
        P(None, TP),
        P(None, TP),
        P(TP),
        P(TP, None),
        P("ep", None),
        P(),
        P("ep", None),
        P("ep", None),
        P("ep", None, TP),
        P("ep", None, TP),
        P("ep", TP, None),
    )
    out_specs = (P("ep", None), P("ep", None))
    return jax.shard_map(program, mesh=split, in_specs=in_specs, out_specs=out_specs, check_vma=False)
```

```python
import jax
import jax.numpy as jnp
from jax import lax
from jax.experimental import pallas as pl
from jax.experimental.pallas import tpu as pltpu
from jax.sharding import Mesh
from jax.sharding import PartitionSpec as P

CONV_CH = 1536
CONV_W = 31
TOP_K = 4
BITS = ("y2", "y1", "y0", "c")
TP = BITS
Y = BITS[:3]
GROUP = 4
EXPERTS = 32


epsilon = 1e-05
clamp_limit = 7.0
swish_slope = 1.702


def shifted(block, axis, distance):
    devices = range(lax.axis_size(axis))
    route = [(i - distance, i) for i in devices if i - distance in devices]
    return lax.ppermute(block, axis, route)


def swapped(x, axis):
    return lax.ppermute(x, axis, [(0, 1), (1, 0)])


def exchanged(x, axis):
    return lax.all_to_all(x, axis, split_axis=0, concat_axis=0, tiled=True)


def core_half(x):
    rows, width = x.shape
    x = x.reshape(2, rows // 2, width)
    own = lax.axis_index("c")
    kept = lax.dynamic_index_in_dim(x, own, 0, keepdims=False)
    given = lax.dynamic_index_in_dim(x, 1 - own, 0, keepdims=False)
    return kept + swapped(given.astype(jnp.bfloat16), "c").astype(jnp.float32)


def totals(halves):
    size = lax.axis_size(Y)
    rows, width = halves[0].shape
    share = rows // size
    parts = [half.astype(jnp.bfloat16).reshape(size, 1, share, width) for half in halves]
    arrived = exchanged(jnp.concatenate(parts, axis=1), Y)
    summed = jnp.sum(arrived.astype(jnp.float32), axis=0).astype(jnp.bfloat16)
    gathered = exchanged(jnp.broadcast_to(summed, (size, *summed.shape)), Y)
    others = swapped(gathered, "c")
    return placed(gathered, others)


def row_norm(inputs, gains):
    widened = inputs.astype(jnp.float32)
    row_mean = jnp.mean(widened, axis=-1, keepdims=True)
    row_var = jnp.mean(jnp.square(widened - row_mean), axis=-1, keepdims=True)
    return (widened - row_mean) * lax.rsqrt(row_var + epsilon) * gains


def convolved(mixer_in, mixer_gain, w_value, w_gate, w_taps):
    normed = row_norm(mixer_in, mixer_gain).astype(jnp.bfloat16)
    values = jnp.dot(normed, w_value, preferred_element_type=jnp.float32)
    gate_pre = jnp.dot(normed, w_gate, preferred_element_type=jnp.float32)
    gated_values = (values * jax.nn.sigmoid(gate_pre)).astype(jnp.bfloat16)
    mixer_rows = gated_values.shape[0]
    reach_rows = CONV_W - 1
    earlier = shifted(gated_values[mixer_rows - reach_rows :], "ep", 1)
    extended = jnp.concatenate([earlier, gated_values], axis=0)
    conv_out = jnp.zeros(gated_values.shape, jnp.float32)
    for offset in range(CONV_W):
        conv_out = (
            conv_out + extended[offset : offset + mixer_rows].astype(jnp.float32) * w_taps[offset]
        )
    return conv_out


def projected(conv_out, channel_gain, w_output):
    sums = jnp.stack([jnp.sum(conv_out, axis=1), jnp.sum(conv_out * conv_out, axis=1)])
    everyone = lax.all_gather(sums, TP)
    sums = jnp.sum(everyone, axis=0)
    row_mean = (sums[0] / CONV_CH)[:, None]
    row_var = (sums[1] / CONV_CH)[:, None] - row_mean * row_mean
    activated = jax.nn.silu(
        (conv_out - row_mean) * lax.rsqrt(row_var + epsilon) * channel_gain
    ).astype(jnp.bfloat16)
    return jnp.dot(activated, w_output, preferred_element_type=jnp.float32)


def places(ids_ref, rows):
    names = lax.broadcasted_iota(jnp.int32, (EXPERTS, rows), 0)
    named = [ids_ref[pl.ds(k, 1), :] == names for k in range(TOP_K)]
    chosen = jnp.zeros((EXPERTS, rows), jnp.float32)
    for k in range(TOP_K):
        chosen = jnp.where(named[k], 1.0, chosen)
    earlier = lax.broadcasted_iota(jnp.int32, (rows, rows), 0)
    later = lax.broadcasted_iota(jnp.int32, (rows, rows), 1)
    before = jnp.where(earlier < later, 1.0, 0.0).astype(jnp.bfloat16)
    rank = jnp.dot(chosen.astype(jnp.bfloat16), before, preferred_element_type=jnp.float32)
    return named, jnp.where(chosen > 0.0, rank, -1.0).astype(jnp.bfloat16)


def spread_over(sent, per_expert):
    of_row = lax.broadcasted_iota(jnp.int32, (sent, EXPERTS), 0) // per_expert
    of_col = lax.broadcasted_iota(jnp.int32, (sent, EXPERTS), 1)
    return jnp.where(of_row == of_col, 1.0, 0.0).astype(jnp.bfloat16)


def taken_by(place, spread, slots, member):
    sent, rows = spread.shape[0], place.shape[1]
    slot = lax.broadcasted_iota(jnp.int32, (sent, rows), 0) % slots * GROUP + member
    return jnp.dot(spread, place, preferred_element_type=jnp.float32) == slot.astype(jnp.float32)


def front_kernel(member, x_ref, gain_ref, ids_ref, rows_ref):
    rows = x_ref.shape[0]
    sent = rows_ref.shape[0]
    slots = sent // EXPERTS
    normed = row_norm(x_ref[...], gain_ref[...]).astype(jnp.bfloat16)
    _, place = places(ids_ref, rows)
    taken = taken_by(place, spread_over(sent, slots), slots, member[0])
    select = jnp.where(taken, 1.0, 0.0).astype(jnp.bfloat16)
    rows_ref[...] = jnp.dot(select, normed, preferred_element_type=jnp.float32).astype(jnp.bfloat16)


def front(member, x, gain, ids, sent):
    _, width = x.shape
    whole = pl.BlockSpec(memory_space=pltpu.VMEM)
    return pl.pallas_call(
        front_kernel,
        in_specs=[pl.BlockSpec(memory_space=pltpu.SMEM)] + [whole] * 3,
        out_specs=whole,
        out_shape=jax.ShapeDtypeStruct((sent, width), jnp.bfloat16),
        compiler_params=pltpu.CompilerParams(vmem_limit_bytes=57000 << 10),
        name="front",
    )(member.reshape(1), x, gain.reshape(1, width), ids)


def mixing_kernel(member, ids_ref, scores_ref, hi_ref, lo_ref):
    sent, rows = hi_ref.shape
    slots = sent // EXPERTS
    raised = [jnp.exp(scores_ref[pl.ds(k, 1), :]) for k in range(TOP_K)]
    total = raised[0] + raised[1] + raised[2] + raised[3]
    named, place = places(ids_ref, rows)
    weights = jnp.zeros((EXPERTS, rows), jnp.float32)
    for k in range(TOP_K):
        weights = jnp.where(named[k], raised[k] / total, weights)
    weights_hi = weights.astype(jnp.bfloat16)
    weights_lo = (weights - weights_hi.astype(jnp.float32)).astype(jnp.bfloat16)
    spread = spread_over(sent, slots)
    taken = taken_by(place, spread, slots, member[0])
    wide_hi = jnp.dot(spread, weights_hi, preferred_element_type=jnp.float32)
    wide_lo = jnp.dot(spread, weights_lo, preferred_element_type=jnp.float32)
    hi_ref[...] = jnp.where(taken, wide_hi, 0.0).astype(jnp.bfloat16)
    lo_ref[...] = jnp.where(taken, wide_lo, 0.0).astype(jnp.bfloat16)


def mixing(member, ids, scores, sent):
    rows = ids.shape[1]
    whole = pl.BlockSpec(memory_space=pltpu.VMEM)
    return pl.pallas_call(
        mixing_kernel,
        in_specs=[pl.BlockSpec(memory_space=pltpu.SMEM)] + [whole] * 2,
        out_specs=[whole] * 2,
        out_shape=[jax.ShapeDtypeStruct((sent, rows), jnp.bfloat16)] * 2,
        compiler_params=pltpu.CompilerParams(vmem_limit_bytes=4 << 20),
        name="mixing",
    )(member.reshape(1), ids, scores)


def hidden_kernel(x_ref, *refs):
    gus, out_ref = refs[:GROUP], refs[GROUP]
    inner = gus[0].shape[1] // 2
    for at, gu in enumerate(gus):
        both = jnp.dot(x_ref[...], gu[...], preferred_element_type=jnp.float32)
        g = jnp.minimum(both[:, :inner], clamp_limit)
        u = jnp.clip(both[:, inner:], -clamp_limit, clamp_limit)
        hidden = (u + 1.0) * g * jax.nn.sigmoid(swish_slope * g)
        out_ref[:, at * inner : (at + 1) * inner] = hidden.astype(jnp.bfloat16)


def down_kernel(hidden_ref, *refs):
    downs, out_hbm, out_buf, sems = refs[:GROUP], refs[GROUP], refs[GROUP + 1], refs[GROUP + 2]
    parts = sems.shape[0]
    step = out_hbm.shape[1] // parts
    copies = []
    for part in range(parts):
        own = pl.ds(part * step, step)
        weights = jnp.concatenate([down[:, own] for down in downs], axis=0)
        out_buf[:, own] = jnp.dot(
            hidden_ref[...], weights, preferred_element_type=jnp.float32
        ).astype(jnp.bfloat16)
        copies.append(pltpu.make_async_copy(out_buf.at[:, own], out_hbm.at[:, own], sems.at[part]))
        copies[-1].start()
    for copy in copies:
        copy.wait()


WHOLE = pl.BlockSpec(memory_space=pltpu.VMEM)
OUTSIDE = pl.BlockSpec(memory_space=pl.ANY)


def hidden_units(x, gus):
    units = GROUP * gus[0].shape[1] // 2
    return pl.pallas_call(
        hidden_kernel,
        in_specs=[WHOLE] * (1 + GROUP),
        out_specs=WHOLE,
        out_shape=jax.ShapeDtypeStruct((x.shape[0], units), jnp.bfloat16),
        compiler_params=pltpu.CompilerParams(vmem_limit_bytes=53000 << 10),
        name="hidden",
    )(x, *gus)


def projected_down(hidden, downs):
    shape = (hidden.shape[0], downs[0].shape[1])
    return pl.pallas_call(
        down_kernel,
        in_specs=[WHOLE] * (1 + GROUP),
        out_specs=OUTSIDE,
        out_shape=jax.ShapeDtypeStruct(shape, jnp.bfloat16),
        scratch_shapes=[pltpu.VMEM(shape, jnp.bfloat16), pltpu.SemaphoreType.DMA((4,))],
        compiler_params=pltpu.CompilerParams(vmem_limit_bytes=53000 << 10),
        name="project",
    )(hidden, *downs)


def placing_kernel(core, own_ref, other_ref, *refs):
    outs, sems = refs[:-1], refs[-1]
    copies = []
    for at, out in enumerate(outs):
        for side, ref in enumerate((own_ref, other_ref)):
            place = core[0] if side == 0 else 1 - core[0]
            copies.append(pltpu.make_async_copy(ref.at[:, at], out.at[place], sems.at[at, side]))
            copies[-1].start()
    for copy in copies:
        copy.wait()


def placed(own, other):
    blocks, count, rows, width = own.shape
    core = lax.axis_index("c").astype(jnp.int32).reshape(1)
    outs = pl.pallas_call(
        placing_kernel,
        in_specs=[pl.BlockSpec(memory_space=pltpu.SMEM), OUTSIDE, OUTSIDE],
        out_specs=[OUTSIDE] * count,
        out_shape=[jax.ShapeDtypeStruct((2, blocks, rows, width), own.dtype)] * count,
        scratch_shapes=[pltpu.SemaphoreType.DMA((count, 2))],
        compiler_params=pltpu.CompilerParams(vmem_limit_bytes=1 << 20),
        name="placing",
    )(core, own, other)
    return [out.reshape(2 * blocks * rows, width) for out in outs]


def program(
    mixer_in,
    mixer_gain,
    w_value,
    w_gate,
    w_taps,
    channel_gain,
    w_output,
    expert_in,
    expert_gain,
    route_experts,
    route_scores,
    expert_gate,
    expert_up,
    expert_down,
):
    rows_b, width = expert_in.shape
    experts = lax.axis_size("ep")
    capacity = 2 * rows_b * TOP_K // experts
    slots = capacity // GROUP
    member = lax.axis_index(("y0", "c")).astype(jnp.int32)

    gate_up = jnp.concatenate([expert_gate[0], expert_up[0]], axis=1)
    down = expert_down[0]
    gu_y = swapped(gate_up, "y0")
    down_y = swapped(down, "y0")
    gu_c = swapped(gate_up, "c")
    down_c = swapped(down, "c")
    gu_d = swapped(gu_y, "c")
    down_d = swapped(down_y, "c")

    ids = route_experts.T
    sending = front(member, expert_in, expert_gain, ids, experts * slots)
    arrived = exchanged(sending.reshape(experts, slots, width), "ep").reshape(-1, width)

    mixing_hi, mixing_lo = mixing(member, ids, route_scores.T, experts * slots)
    conv_out = convolved(mixer_in, mixer_gain, w_value, w_gate, w_taps)
    mixer_partial = projected(conv_out, channel_gain, w_output)
    mixer_half = core_half(mixer_partial)

    hidden = hidden_units(arrived, (gate_up, gu_c, gu_y, gu_d))
    partial = projected_down(hidden, (down, down_c, down_y, down_d))
    returned = exchanged(partial.reshape(experts, slots, width), "ep").reshape(-1, width)

    def mixed(m):
        return lax.dot_general(
            m, returned, (((0,), (0,)), ((), ())), preferred_element_type=jnp.float32
        )

    expert_half = core_half(mixed(mixing_hi) + mixed(mixing_lo))
    mixer_out, expert_out = totals([mixer_half, expert_half])
    return (mixer_out, expert_out)


def solution(mesh):
    split = Mesh(mesh.devices.reshape(mesh.shape["ep"], 2, 2, 2, 2), ("ep", *TP))
    in_specs = (
        P("ep", None),
        P(),
        P(None, TP),
        P(None, TP),
        P(None, TP),
        P(TP),
        P(TP, None),
        P("ep", None),
        P(),
        P("ep", None),
        P("ep", None),
        P("ep", None, TP),
        P("ep", None, TP),
        P("ep", TP, None),
    )
    out_specs = (P("ep", None), P("ep", None))
    return jax.shard_map(program, mesh=split, in_specs=in_specs, out_specs=out_specs, check_vma=False)
```

```python
import jax
import jax.numpy as jnp
from jax import lax
from jax.experimental import pallas as pl
from jax.experimental.pallas import tpu as pltpu
from jax.sharding import Mesh
from jax.sharding import PartitionSpec as P

CONV_CH = 1536
CONV_W = 31
TOP_K = 4
BITS = ("y2", "y1", "y0", "c")
TP = BITS
Y = BITS[:3]
GROUP = 4
EXPERTS = 32


epsilon = 1e-05
clamp_limit = 7.0
swish_slope = 1.702


def shifted(block, axis, distance):
    devices = range(lax.axis_size(axis))
    route = [(i - distance, i) for i in devices if i - distance in devices]
    return lax.ppermute(block, axis, route)


def swapped(x, axis):
    return lax.ppermute(x, axis, [(0, 1), (1, 0)])


def exchanged(x, axis):
    return lax.all_to_all(x, axis, split_axis=0, concat_axis=0, tiled=True)


def core_half(x):
    rows, width = x.shape
    x = x.reshape(2, rows // 2, width)
    own = lax.axis_index("c")
    kept = lax.dynamic_index_in_dim(x, own, 0, keepdims=False)
    given = lax.dynamic_index_in_dim(x, 1 - own, 0, keepdims=False)
    return kept + swapped(given.astype(jnp.bfloat16), "c").astype(jnp.float32)


def totals(halves):
    size = lax.axis_size(Y)
    rows, width = halves[0].shape
    share = rows // size
    parts = [half.astype(jnp.bfloat16).reshape(size, 1, share, width) for half in halves]
    arrived = exchanged(jnp.concatenate(parts, axis=1), Y)
    summed = jnp.sum(arrived.astype(jnp.float32), axis=0).astype(jnp.bfloat16)
    gathered = exchanged(jnp.broadcast_to(summed, (size, *summed.shape)), Y)
    others = swapped(gathered, "c")
    return placed(gathered, others)


def row_norm(inputs, gains):
    widened = inputs.astype(jnp.float32)
    row_mean = jnp.mean(widened, axis=-1, keepdims=True)
    row_var = jnp.mean(jnp.square(widened - row_mean), axis=-1, keepdims=True)
    return (widened - row_mean) * lax.rsqrt(row_var + epsilon) * gains


def convolved(mixer_in, mixer_gain, w_value, w_gate, w_taps):
    normed = row_norm(mixer_in, mixer_gain).astype(jnp.bfloat16)
    values = jnp.dot(normed, w_value, preferred_element_type=jnp.float32)
    gate_pre = jnp.dot(normed, w_gate, preferred_element_type=jnp.float32)
    gated_values = (values * jax.nn.sigmoid(gate_pre)).astype(jnp.bfloat16)
    mixer_rows = gated_values.shape[0]
    reach_rows = CONV_W - 1
    earlier = shifted(gated_values[mixer_rows - reach_rows :], "ep", 1)
    extended = jnp.concatenate([earlier, gated_values], axis=0)
    conv_out = jnp.zeros(gated_values.shape, jnp.float32)
    for offset in range(CONV_W):
        conv_out = (
            conv_out + extended[offset : offset + mixer_rows].astype(jnp.float32) * w_taps[offset]
        )
    return conv_out


def projected(conv_out, channel_gain, w_output):
    sums = jnp.stack([jnp.sum(conv_out, axis=1), jnp.sum(conv_out * conv_out, axis=1)])
    everyone = lax.all_gather(sums, TP)
    sums = jnp.sum(everyone, axis=0)
    row_mean = (sums[0] / CONV_CH)[:, None]
    row_var = (sums[1] / CONV_CH)[:, None] - row_mean * row_mean
    activated = jax.nn.silu(
        (conv_out - row_mean) * lax.rsqrt(row_var + epsilon) * channel_gain
    ).astype(jnp.bfloat16)
    return jnp.dot(activated, w_output, preferred_element_type=jnp.float32)


def places(ids_ref, rows):
    names = lax.broadcasted_iota(jnp.int32, (EXPERTS, rows), 0)
    named = [ids_ref[pl.ds(k, 1), :] == names for k in range(TOP_K)]
    chosen = jnp.zeros((EXPERTS, rows), jnp.float32)
    for k in range(TOP_K):
        chosen = jnp.where(named[k], 1.0, chosen)
    earlier = lax.broadcasted_iota(jnp.int32, (rows, rows), 0)
    later = lax.broadcasted_iota(jnp.int32, (rows, rows), 1)
    before = jnp.where(earlier < later, 1.0, 0.0).astype(jnp.bfloat16)
    rank = jnp.dot(chosen.astype(jnp.bfloat16), before, preferred_element_type=jnp.float32)
    return named, jnp.where(chosen > 0.0, rank, -1.0).astype(jnp.bfloat16)


def spread_over(sent, per_expert):
    of_row = lax.broadcasted_iota(jnp.int32, (sent, EXPERTS), 0) // per_expert
    of_col = lax.broadcasted_iota(jnp.int32, (sent, EXPERTS), 1)
    return jnp.where(of_row == of_col, 1.0, 0.0).astype(jnp.bfloat16)


def taken_by(place, spread, slots, member):
    sent, rows = spread.shape[0], place.shape[1]
    slot = lax.broadcasted_iota(jnp.int32, (sent, rows), 0) % slots * GROUP + member
    return jnp.dot(spread, place, preferred_element_type=jnp.float32) == slot.astype(jnp.float32)


def front_kernel(member, x_ref, gain_ref, ids_ref, rows_ref):
    rows = x_ref.shape[0]
    sent = rows_ref.shape[0]
    slots = sent // EXPERTS
    normed = row_norm(x_ref[...], gain_ref[...]).astype(jnp.bfloat16)
    _, place = places(ids_ref, rows)
    taken = taken_by(place, spread_over(sent, slots), slots, member[0])
    select = jnp.where(taken, 1.0, 0.0).astype(jnp.bfloat16)
    rows_ref[...] = jnp.dot(select, normed, preferred_element_type=jnp.float32).astype(jnp.bfloat16)


def front(member, x, gain, ids, sent):
    _, width = x.shape
    whole = pl.BlockSpec(memory_space=pltpu.VMEM)
    return pl.pallas_call(
        front_kernel,
        in_specs=[pl.BlockSpec(memory_space=pltpu.SMEM)] + [whole] * 3,
        out_specs=whole,
        out_shape=jax.ShapeDtypeStruct((sent, width), jnp.bfloat16),
        compiler_params=pltpu.CompilerParams(vmem_limit_bytes=57000 << 10),
        name="front",
    )(member.reshape(1), x, gain.reshape(1, width), ids)


def mixing_kernel(member, ids_ref, scores_ref, hi_ref, lo_ref):
    sent, rows = hi_ref.shape
    slots = sent // EXPERTS
    raised = [jnp.exp(scores_ref[pl.ds(k, 1), :]) for k in range(TOP_K)]
    total = raised[0] + raised[1] + raised[2] + raised[3]
    named, place = places(ids_ref, rows)
    weights = jnp.zeros((EXPERTS, rows), jnp.float32)
    for k in range(TOP_K):
        weights = jnp.where(named[k], raised[k] / total, weights)
    weights_hi = weights.astype(jnp.bfloat16)
    weights_lo = (weights - weights_hi.astype(jnp.float32)).astype(jnp.bfloat16)
    spread = spread_over(sent, slots)
    taken = taken_by(place, spread, slots, member[0])
    wide_hi = jnp.dot(spread, weights_hi, preferred_element_type=jnp.float32)
    wide_lo = jnp.dot(spread, weights_lo, preferred_element_type=jnp.float32)
    hi_ref[...] = jnp.where(taken, wide_hi, 0.0).astype(jnp.bfloat16)
    lo_ref[...] = jnp.where(taken, wide_lo, 0.0).astype(jnp.bfloat16)


def mixing(member, ids, scores, sent):
    rows = ids.shape[1]
    whole = pl.BlockSpec(memory_space=pltpu.VMEM)
    return pl.pallas_call(
        mixing_kernel,
        in_specs=[pl.BlockSpec(memory_space=pltpu.SMEM)] + [whole] * 2,
        out_specs=[whole] * 2,
        out_shape=[jax.ShapeDtypeStruct((sent, rows), jnp.bfloat16)] * 2,
        compiler_params=pltpu.CompilerParams(vmem_limit_bytes=4 << 20),
        name="mixing",
    )(member.reshape(1), ids, scores)


def hidden_kernel(x_ref, *refs):
    gus, out_ref = refs[:GROUP], refs[GROUP]
    inner = gus[0].shape[1] // 2
    for at, gu in enumerate(gus):
        both = jnp.dot(x_ref[...], gu[...], preferred_element_type=jnp.float32)
        g = jnp.minimum(both[:, :inner], clamp_limit)
        u = jnp.clip(both[:, inner:], -clamp_limit, clamp_limit)
        hidden = (u + 1.0) * g * jax.nn.sigmoid(swish_slope * g)
        out_ref[:, at * inner : (at + 1) * inner] = hidden.astype(jnp.bfloat16)


def down_kernel(hidden_ref, *refs):
    downs, out_hbm, out_buf, sems = refs[:GROUP], refs[GROUP], refs[GROUP + 1], refs[GROUP + 2]
    parts = sems.shape[0]
    step = out_hbm.shape[1] // parts
    copies = []
    for part in range(parts):
        own = pl.ds(part * step, step)
        weights = jnp.concatenate([down[:, own] for down in downs], axis=0)
        out_buf[:, own] = jnp.dot(
            hidden_ref[...], weights, preferred_element_type=jnp.float32
        ).astype(jnp.bfloat16)
        copies.append(pltpu.make_async_copy(out_buf.at[:, own], out_hbm.at[:, own], sems.at[part]))
        copies[-1].start()
    for copy in copies:
        copy.wait()


WHOLE = pl.BlockSpec(memory_space=pltpu.VMEM)
OUTSIDE = pl.BlockSpec(memory_space=pl.ANY)


def hidden_units(x, gus):
    units = GROUP * gus[0].shape[1] // 2
    return pl.pallas_call(
        hidden_kernel,
        in_specs=[WHOLE] * (1 + GROUP),
        out_specs=WHOLE,
        out_shape=jax.ShapeDtypeStruct((x.shape[0], units), jnp.bfloat16),
        compiler_params=pltpu.CompilerParams(vmem_limit_bytes=53000 << 10),
        name="hidden",
    )(x, *gus)


def projected_down(hidden, downs):
    shape = (hidden.shape[0], downs[0].shape[1])
    return pl.pallas_call(
        down_kernel,
        in_specs=[WHOLE] * (1 + GROUP),
        out_specs=OUTSIDE,
        out_shape=jax.ShapeDtypeStruct(shape, jnp.bfloat16),
        scratch_shapes=[pltpu.VMEM(shape, jnp.bfloat16), pltpu.SemaphoreType.DMA((4,))],
        compiler_params=pltpu.CompilerParams(vmem_limit_bytes=53000 << 10),
        name="project",
    )(hidden, *downs)


def placing_kernel(core, own_ref, other_ref, *refs):
    outs, sems = refs[:-1], refs[-1]
    copies = []
    for at, out in enumerate(outs):
        for side, ref in enumerate((own_ref, other_ref)):
            place = core[0] if side == 0 else 1 - core[0]
            copies.append(pltpu.make_async_copy(ref.at[:, at], out.at[place], sems.at[at, side]))
            copies[-1].start()
    for copy in copies:
        copy.wait()


def placed(own, other):
    blocks, count, rows, width = own.shape
    core = lax.axis_index("c").astype(jnp.int32).reshape(1)
    outs = pl.pallas_call(
        placing_kernel,
        in_specs=[pl.BlockSpec(memory_space=pltpu.SMEM), OUTSIDE, OUTSIDE],
        out_specs=[OUTSIDE] * count,
        out_shape=[jax.ShapeDtypeStruct((2, blocks, rows, width), own.dtype)] * count,
        scratch_shapes=[pltpu.SemaphoreType.DMA((count, 2))],
        compiler_params=pltpu.CompilerParams(vmem_limit_bytes=1 << 20),
        name="placing",
    )(core, own, other)
    return [out.reshape(2 * blocks * rows, width) for out in outs]


def program(
    mixer_in,
    mixer_gain,
    w_value,
    w_gate,
    w_taps,
    channel_gain,
    w_output,
    expert_in,
    expert_gain,
    route_experts,
    route_scores,
    expert_gate,
    expert_up,
    expert_down,
):
    rows_b, width = expert_in.shape
    experts = lax.axis_size("ep")
    capacity = 2 * rows_b * TOP_K // experts
    slots = capacity // GROUP
    member = lax.axis_index(("y0", "c")).astype(jnp.int32)

    gate, up, down = expert_gate[0], expert_up[0], expert_down[0]
    gate_y = swapped(gate, "y0")
    up_y = swapped(up, "y0")
    down_y = swapped(down, "y0")
    packed = jnp.concatenate([gate, up], axis=1)
    gu_c = swapped(packed, "c")
    down_c = swapped(down, "c")
    packed_y = jnp.concatenate([gate_y, up_y], axis=1)
    gu_d = swapped(packed_y, "c")
    down_d = swapped(down_y, "c")

    ids = route_experts.T
    sending = front(member, expert_in, expert_gain, ids, experts * slots)
    arrived = exchanged(sending.reshape(experts, slots, width), "ep").reshape(-1, width)

    mixing_hi, mixing_lo = mixing(member, ids, route_scores.T, experts * slots)
    conv_out = convolved(mixer_in, mixer_gain, w_value, w_gate, w_taps)
    mixer_partial = projected(conv_out, channel_gain, w_output)
    mixer_half = core_half(mixer_partial)

    hidden = hidden_units(arrived, (packed, gu_c, packed_y, gu_d))
    partial = projected_down(hidden, (down, down_c, down_y, down_d))
    returned = exchanged(partial.reshape(experts, slots, width), "ep").reshape(-1, width)

    def mixed(m):
        return lax.dot_general(
            m, returned, (((0,), (0,)), ((), ())), preferred_element_type=jnp.float32
        )

    expert_half = core_half(mixed(mixing_hi) + mixed(mixing_lo))
    mixer_out, expert_out = totals([mixer_half, expert_half])
    return (mixer_out, expert_out)


def solution(mesh):
    split = Mesh(mesh.devices.reshape(mesh.shape["ep"], 2, 2, 2, 2), ("ep", *TP))
    in_specs = (
        P("ep", None),
        P(),
        P(None, TP),
        P(None, TP),
        P(None, TP),
        P(TP),
        P(TP, None),
        P("ep", None),
        P(),
        P("ep", None),
        P("ep", None),
        P("ep", None, TP),
        P("ep", None, TP),
        P("ep", TP, None),
    )
    out_specs = (P("ep", None), P("ep", None))
    return jax.shard_map(program, mesh=split, in_specs=in_specs, out_specs=out_specs, check_vma=False)
```

```python
import jax
import jax.numpy as jnp
from jax import lax
from jax.experimental import pallas as pl
from jax.experimental.pallas import tpu as pltpu
from jax.sharding import Mesh
from jax.sharding import PartitionSpec as P

CONV_CH = 1536
CONV_W = 31
TOP_K = 4
BITS = ("y2", "y1", "y0", "c")
TP = BITS
Y = BITS[:3]
GROUP = 4
EXPERTS = 32


epsilon = 1e-05
clamp_limit = 7.0
swish_slope = 1.702


def shifted(block, axis, distance):
    devices = range(lax.axis_size(axis))
    route = [(i - distance, i) for i in devices if i - distance in devices]
    return lax.ppermute(block, axis, route)


def swapped(x, axis):
    return lax.ppermute(x, axis, [(0, 1), (1, 0)])


def exchanged(x, axis):
    return lax.all_to_all(x, axis, split_axis=0, concat_axis=0, tiled=True)


def core_half(x):
    rows, width = x.shape
    x = x.reshape(2, rows // 2, width)
    own = lax.axis_index("c")
    kept = lax.dynamic_index_in_dim(x, own, 0, keepdims=False)
    given = lax.dynamic_index_in_dim(x, 1 - own, 0, keepdims=False)
    return kept + swapped(given.astype(jnp.bfloat16), "c").astype(jnp.float32)


def totals(halves):
    size = lax.axis_size(Y)
    rows, width = halves[0].shape
    share = rows // size
    parts = [half.astype(jnp.bfloat16).reshape(size, 1, share, width) for half in halves]
    arrived = exchanged(jnp.concatenate(parts, axis=1), Y)
    summed = jnp.sum(arrived.astype(jnp.float32), axis=0).astype(jnp.bfloat16)
    gathered = exchanged(jnp.broadcast_to(summed, (size, *summed.shape)), Y)
    others = swapped(gathered, "c")
    return placed(gathered, others)


def row_norm(inputs, gains):
    widened = inputs.astype(jnp.float32)
    row_mean = jnp.mean(widened, axis=-1, keepdims=True)
    row_var = jnp.mean(jnp.square(widened - row_mean), axis=-1, keepdims=True)
    return (widened - row_mean) * lax.rsqrt(row_var + epsilon) * gains


def convolved(mixer_in, mixer_gain, w_value, w_gate, w_taps):
    normed = row_norm(mixer_in, mixer_gain).astype(jnp.bfloat16)
    values = jnp.dot(normed, w_value, preferred_element_type=jnp.float32)
    gate_pre = jnp.dot(normed, w_gate, preferred_element_type=jnp.float32)
    gated_values = (values * jax.nn.sigmoid(gate_pre)).astype(jnp.bfloat16)
    mixer_rows = gated_values.shape[0]
    reach_rows = CONV_W - 1
    earlier = shifted(gated_values[mixer_rows - reach_rows :], "ep", 1)
    extended = jnp.concatenate([earlier, gated_values], axis=0)
    conv_out = jnp.zeros(gated_values.shape, jnp.float32)
    for offset in range(CONV_W):
        conv_out = (
            conv_out + extended[offset : offset + mixer_rows].astype(jnp.float32) * w_taps[offset]
        )
    return conv_out


def projected(conv_out, channel_gain, w_output):
    sums = jnp.stack([jnp.sum(conv_out, axis=1), jnp.sum(conv_out * conv_out, axis=1)])
    everyone = lax.all_gather(sums, TP)
    sums = jnp.sum(everyone, axis=0)
    row_mean = (sums[0] / CONV_CH)[:, None]
    row_var = (sums[1] / CONV_CH)[:, None] - row_mean * row_mean
    activated = jax.nn.silu(
        (conv_out - row_mean) * lax.rsqrt(row_var + epsilon) * channel_gain
    ).astype(jnp.bfloat16)
    return jnp.dot(activated, w_output, preferred_element_type=jnp.float32)


def places(ids_ref, rows):
    names = lax.broadcasted_iota(jnp.int32, (EXPERTS, rows), 0)
    named = [ids_ref[pl.ds(k, 1), :] == names for k in range(TOP_K)]
    chosen = jnp.zeros((EXPERTS, rows), jnp.float32)
    for k in range(TOP_K):
        chosen = jnp.where(named[k], 1.0, chosen)
    earlier = lax.broadcasted_iota(jnp.int32, (rows, rows), 0)
    later = lax.broadcasted_iota(jnp.int32, (rows, rows), 1)
    before = jnp.where(earlier < later, 1.0, 0.0).astype(jnp.bfloat16)
    rank = jnp.dot(chosen.astype(jnp.bfloat16), before, preferred_element_type=jnp.float32)
    return named, jnp.where(chosen > 0.0, rank, -1.0).astype(jnp.bfloat16)


def spread_over(sent, per_expert):
    of_row = lax.broadcasted_iota(jnp.int32, (sent, EXPERTS), 0) // per_expert
    of_col = lax.broadcasted_iota(jnp.int32, (sent, EXPERTS), 1)
    return jnp.where(of_row == of_col, 1.0, 0.0).astype(jnp.bfloat16)


def taken_by(place, spread, slots, member):
    sent, rows = spread.shape[0], place.shape[1]
    slot = lax.broadcasted_iota(jnp.int32, (sent, rows), 0) % slots * GROUP + member
    return jnp.dot(spread, place, preferred_element_type=jnp.float32) == slot.astype(jnp.float32)


def front_kernel(member, x_ref, gain_ref, ids_ref, out_hbm, out_buf, sems):
    rows = x_ref.shape[0]
    sent, width = out_hbm.shape
    slots = sent // EXPERTS
    normed = row_norm(x_ref[...], gain_ref[...]).astype(jnp.bfloat16)
    _, place = places(ids_ref, rows)
    taken = taken_by(place, spread_over(sent, slots), slots, member[0])
    select = jnp.where(taken, 1.0, 0.0).astype(jnp.bfloat16)
    parts = sems.shape[0]
    step = width // parts
    copies = []
    for part in range(parts):
        own = slice(part * step, (part + 1) * step)
        out_buf[:, own] = jnp.dot(
            select, normed[:, own], preferred_element_type=jnp.float32
        ).astype(jnp.bfloat16)
        copies.append(pltpu.make_async_copy(out_buf.at[:, own], out_hbm.at[:, own], sems.at[part]))
        copies[-1].start()
    for copy in copies:
        copy.wait()


def front(member, x, gain, ids, sent):
    _, width = x.shape
    whole = pl.BlockSpec(memory_space=pltpu.VMEM)
    return pl.pallas_call(
        front_kernel,
        in_specs=[pl.BlockSpec(memory_space=pltpu.SMEM)] + [whole] * 3,
        out_specs=pl.BlockSpec(memory_space=pl.ANY),
        out_shape=jax.ShapeDtypeStruct((sent, width), jnp.bfloat16),
        scratch_shapes=[pltpu.VMEM((sent, width), jnp.bfloat16), pltpu.SemaphoreType.DMA((4,))],
        compiler_params=pltpu.CompilerParams(vmem_limit_bytes=57000 << 10),
        name="front",
    )(member.reshape(1), x, gain.reshape(1, width), ids)


def mixing_kernel(member, ids_ref, scores_ref, hi_ref, lo_ref):
    sent, rows = hi_ref.shape
    slots = sent // EXPERTS
    raised = [jnp.exp(scores_ref[pl.ds(k, 1), :]) for k in range(TOP_K)]
    total = raised[0] + raised[1] + raised[2] + raised[3]
    named, place = places(ids_ref, rows)
    weights = jnp.zeros((EXPERTS, rows), jnp.float32)
    for k in range(TOP_K):
        weights = jnp.where(named[k], raised[k] / total, weights)
    weights_hi = weights.astype(jnp.bfloat16)
    weights_lo = (weights - weights_hi.astype(jnp.float32)).astype(jnp.bfloat16)
    spread = spread_over(sent, slots)
    taken = taken_by(place, spread, slots, member[0])
    wide_hi = jnp.dot(spread, weights_hi, preferred_element_type=jnp.float32)
    wide_lo = jnp.dot(spread, weights_lo, preferred_element_type=jnp.float32)
    hi_ref[...] = jnp.where(taken, wide_hi, 0.0).astype(jnp.bfloat16)
    lo_ref[...] = jnp.where(taken, wide_lo, 0.0).astype(jnp.bfloat16)


def mixing(member, ids, scores, sent):
    rows = ids.shape[1]
    whole = pl.BlockSpec(memory_space=pltpu.VMEM)
    return pl.pallas_call(
        mixing_kernel,
        in_specs=[pl.BlockSpec(memory_space=pltpu.SMEM)] + [whole] * 2,
        out_specs=[whole] * 2,
        out_shape=[jax.ShapeDtypeStruct((sent, rows), jnp.bfloat16)] * 2,
        compiler_params=pltpu.CompilerParams(vmem_limit_bytes=4 << 20),
        name="mixing",
    )(member.reshape(1), ids, scores)


def hidden_kernel(x_ref, *refs):
    gus, out_ref = refs[:GROUP], refs[GROUP]
    inner = gus[0].shape[1] // 2
    for at, gu in enumerate(gus):
        both = jnp.dot(x_ref[...], gu[...], preferred_element_type=jnp.float32)
        g = jnp.minimum(both[:, :inner], clamp_limit)
        u = jnp.clip(both[:, inner:], -clamp_limit, clamp_limit)
        hidden = (u + 1.0) * g * jax.nn.sigmoid(swish_slope * g)
        out_ref[:, at * inner : (at + 1) * inner] = hidden.astype(jnp.bfloat16)


def down_kernel(hidden_ref, *refs):
    downs, out_hbm, out_buf, sems = refs[:GROUP], refs[GROUP], refs[GROUP + 1], refs[GROUP + 2]
    parts = sems.shape[0]
    step = out_hbm.shape[1] // parts
    copies = []
    for part in range(parts):
        own = pl.ds(part * step, step)
        weights = jnp.concatenate([down[:, own] for down in downs], axis=0)
        out_buf[:, own] = jnp.dot(
            hidden_ref[...], weights, preferred_element_type=jnp.float32
        ).astype(jnp.bfloat16)
        copies.append(pltpu.make_async_copy(out_buf.at[:, own], out_hbm.at[:, own], sems.at[part]))
        copies[-1].start()
    for copy in copies:
        copy.wait()


WHOLE = pl.BlockSpec(memory_space=pltpu.VMEM)
OUTSIDE = pl.BlockSpec(memory_space=pl.ANY)


def hidden_units(x, gus):
    units = GROUP * gus[0].shape[1] // 2
    return pl.pallas_call(
        hidden_kernel,
        in_specs=[WHOLE] * (1 + GROUP),
        out_specs=WHOLE,
        out_shape=jax.ShapeDtypeStruct((x.shape[0], units), jnp.bfloat16),
        compiler_params=pltpu.CompilerParams(vmem_limit_bytes=53000 << 10),
        name="hidden",
    )(x, *gus)


def projected_down(hidden, downs):
    shape = (hidden.shape[0], downs[0].shape[1])
    return pl.pallas_call(
        down_kernel,
        in_specs=[WHOLE] * (1 + GROUP),
        out_specs=OUTSIDE,
        out_shape=jax.ShapeDtypeStruct(shape, jnp.bfloat16),
        scratch_shapes=[pltpu.VMEM(shape, jnp.bfloat16), pltpu.SemaphoreType.DMA((4,))],
        compiler_params=pltpu.CompilerParams(vmem_limit_bytes=53000 << 10),
        name="project",
    )(hidden, *downs)


def placing_kernel(core, own_ref, other_ref, *refs):
    outs, sems = refs[:-1], refs[-1]
    copies = []
    for at, out in enumerate(outs):
        for side, ref in enumerate((own_ref, other_ref)):
            place = core[0] if side == 0 else 1 - core[0]
            copies.append(pltpu.make_async_copy(ref.at[:, at], out.at[place], sems.at[at, side]))
            copies[-1].start()
    for copy in copies:
        copy.wait()


def placed(own, other):
    blocks, count, rows, width = own.shape
    core = lax.axis_index("c").astype(jnp.int32).reshape(1)
    outs = pl.pallas_call(
        placing_kernel,
        in_specs=[pl.BlockSpec(memory_space=pltpu.SMEM), OUTSIDE, OUTSIDE],
        out_specs=[OUTSIDE] * count,
        out_shape=[jax.ShapeDtypeStruct((2, blocks, rows, width), own.dtype)] * count,
        scratch_shapes=[pltpu.SemaphoreType.DMA((count, 2))],
        compiler_params=pltpu.CompilerParams(vmem_limit_bytes=1 << 20),
        name="placing",
    )(core, own, other)
    return [out.reshape(2 * blocks * rows, width) for out in outs]


def program(
    mixer_in,
    mixer_gain,
    w_value,
    w_gate,
    w_taps,
    channel_gain,
    w_output,
    expert_in,
    expert_gain,
    route_experts,
    route_scores,
    expert_gate,
    expert_up,
    expert_down,
):
    rows_b, width = expert_in.shape
    experts = lax.axis_size("ep")
    capacity = 2 * rows_b * TOP_K // experts
    slots = capacity // GROUP
    member = lax.axis_index(("y0", "c")).astype(jnp.int32)

    gate, up, down = expert_gate[0], expert_up[0], expert_down[0]
    gate_y = swapped(gate, "y0")
    up_y = swapped(up, "y0")
    down_y = swapped(down, "y0")
    packed = jnp.concatenate([gate, up], axis=1)
    gu_c = swapped(packed, "c")
    down_c = swapped(down, "c")
    packed_y = jnp.concatenate([gate_y, up_y], axis=1)
    gu_d = swapped(packed_y, "c")
    down_d = swapped(down_y, "c")

    ids = route_experts.T
    sending = front(member, expert_in, expert_gain, ids, experts * slots)
    arrived = exchanged(sending.reshape(experts, slots, width), "ep").reshape(-1, width)

    mixing_hi, mixing_lo = mixing(member, ids, route_scores.T, experts * slots)
    conv_out = convolved(mixer_in, mixer_gain, w_value, w_gate, w_taps)
    mixer_partial = projected(conv_out, channel_gain, w_output)
    mixer_half = core_half(mixer_partial)

    hidden = hidden_units(arrived, (packed, gu_c, packed_y, gu_d))
    partial = projected_down(hidden, (down, down_c, down_y, down_d))
    returned = exchanged(partial.reshape(experts, slots, width), "ep").reshape(-1, width)

    def mixed(m):
        return lax.dot_general(
            m, returned, (((0,), (0,)), ((), ())), preferred_element_type=jnp.float32
        )

    expert_half = core_half(mixed(mixing_hi) + mixed(mixing_lo))
    mixer_out, expert_out = totals([mixer_half, expert_half])
    return (mixer_out, expert_out)


def solution(mesh):
    split = Mesh(mesh.devices.reshape(mesh.shape["ep"], 2, 2, 2, 2), ("ep", *TP))
    in_specs = (
        P("ep", None),
        P(),
        P(None, TP),
        P(None, TP),
        P(None, TP),
        P(TP),
        P(TP, None),
        P("ep", None),
        P(),
        P("ep", None),
        P("ep", None),
        P("ep", None, TP),
        P("ep", None, TP),
        P("ep", TP, None),
    )
    out_specs = (P("ep", None), P("ep", None))
    return jax.shard_map(program, mesh=split, in_specs=in_specs, out_specs=out_specs, check_vma=False)
```
